32 devices in a mesh: sp: 4 (over x, core), dp: 8 (over z, y).
Axes of the slice: x: 2, y: 2, z: 4, core: 2. Of those that a mesh axis runs over, the one named last changes fastest.
Arguments:
- cotangent: bfloat16 [8, 512, 2048], P('dp', 'sp'), may hold values from -6 to 6
- layer_input: bfloat16 [8, 512, 2048], P('dp', 'sp'), may hold values from -6 to 6
- x_pre: bfloat16 [8, 512, 2048], P('dp', None, 'sp'), may hold values from -6 to 6
- z_pre: bfloat16 [8, 512, 2048], P('dp', None, 'sp'), may hold values from -6 to 6
- b_pre: bfloat16 [8, 512, 256], P('dp'), may hold values from -6 to 6
- c_pre: bfloat16 [8, 512, 256], P('dp'), may hold values from -6 to 6
- dt_raw: bfloat16 [8, 512, 32], P('dp', None, 'sp'), may hold values from -4.4 to 11.4
- conv_x: bfloat16 [4, 2048], P(None, 'sp'), may hold values from -3 to 3
- conv_b: bfloat16 [4, 256], replicated, may hold values from -3 to 3
- conv_c: bfloat16 [4, 256], replicated, may hold values from -3 to 3
- dt_bias: float32 [32], P('sp'), may hold values from -3.8 to -3.2
- a_log: float32 [32], P('sp'), may hold values from -9 to 0.5
- d_skip: float32 [32], P('sp'), may hold values from 0.5 to 1.5
- norm_w: float32 [2048], P('sp'), may hold values from 0.1 to 1.9
Outputs:
- d_x_pre: bfloat16 [8, 512, 2048], P('dp', 'sp')
- d_z_pre: bfloat16 [8, 512, 2048], P('dp', 'sp')
- d_b_pre: bfloat16 [8, 512, 256], P('dp', 'sp')
- d_c_pre: bfloat16 [8, 512, 256], P('dp', 'sp')
- d_dt_raw: bfloat16 [8, 512, 32], P('dp', 'sp')
- grad_a_log: float32 [32], P('sp')
- grad_w_dt: float32 [2048, 32], replicated
The draws below stay inside these ranges and needn't reach their ends.
All inputs are finite; a program needn't handle non-finite values.
Results may differ from the reference program's by a relative error of at most 0.017.
Values may be sent and summed in bfloat16 or wider, within the bound.
A program may use at most 128 MiB of HBM per device.

```python
import jax
import jax.numpy as jnp
from jax import lax

D = 2048
HEADS = 32
HEAD_DIM = 64
GROUPS = 2
STATE = 128
CONV = 4
BLOCK = 128
TOK_DEV = 128
SEQ_LEN = 512
NUM_STREAMS = 8
N_SP = 4


def draw_a_log(key, part):
    pick_key, spread_key = jax.random.split(jax.random.fold_in(key, 11))
    ranking = jax.random.permutation(pick_key, HEADS)
    gradual_decay_heads = ranking < HEADS // 2
    spread_draw = jax.random.uniform(spread_key, (HEADS,), jnp.float32)
    slow_rate = jnp.exp(jnp.log(0.3) + spread_draw * jnp.log(4.0)) / (TOK_DEV * N_SP)
    fast_rate = jnp.exp(jnp.log(1.0 / 60.0) + spread_draw * jnp.log(2.0))
    return jnp.log(jnp.where(gradual_decay_heads, slow_rate, fast_rate) / 0.03).astype(jnp.float32)


def draw_dt_raw(key, part):
    derived_prng_seeds = jax.random.split(jax.random.fold_in(key, 23), 3)
    overall_span_tokens = TOK_DEV * N_SP
    jitter = 0.6 * jnp.clip(jax.random.normal(derived_prng_seeds[0], (NUM_STREAMS, overall_span_tokens, HEADS), jnp.float32), -6.0, 6.0)
    block_level = jax.random.uniform(derived_prng_seeds[1], (NUM_STREAMS, N_SP, 1, HEADS), jnp.float32, minval=-0.7, maxval=0.7)
    offsets = jnp.broadcast_to(block_level, (NUM_STREAMS, N_SP, TOK_DEV, HEADS)).reshape(NUM_STREAMS, overall_span_tokens, HEADS)
    clustered_bundles = jax.random.randint(derived_prng_seeds[2], (NUM_STREAMS, 3), 0, overall_span_tokens)
    placement_indices = jnp.arange(overall_span_tokens)
    flagged_elements = jnp.any(placement_indices[None, :, None] == clustered_bundles[:, None, :], axis=2).astype(jnp.float32)
    return (jitter + offsets + 7.0 * flagged_elements[:, :, None]).astype(jnp.bfloat16)


def level_of(key, dims, cuts, low, largest):
    gain = 1.0
    for position, parts in cuts:
        steps = jax.random.uniform(jax.random.fold_in(jax.random.fold_in(key, 6), position), (parts,), jnp.float32, low / len(cuts), largest / len(cuts))
        gain = gain * jnp.repeat(jnp.exp(steps), dims[position] // parts).reshape((-1,) + (1,) * (len(dims) - 1 - position))
    return gain


def centred(stream_key, dims, width, reach, shards=(), held_as=jnp.bfloat16):
    level = level_of(stream_key, dims, shards, -0.22, 0.18) if shards else 1.0
    result = jax.random.normal(stream_key, dims, jnp.float32) * width * level
    return jnp.minimum(jnp.maximum(result, -reach), reach).astype(held_as)


def setup_inputs(seed: int = 0) -> dict:
    streams_of = jax.random.split(jax.random.key(seed), 15)
    return {
        "cotangent": centred(streams_of[0], (NUM_STREAMS, SEQ_LEN, HEADS * HEAD_DIM), 1.0, 6.0, ((0, 8), (1, 4))),
        "layer_input": centred(streams_of[1], (NUM_STREAMS, SEQ_LEN, D), 1.0, 6.0, ((0, 8), (1, 4))),
        "x_pre": centred(streams_of[2], (NUM_STREAMS, SEQ_LEN, HEADS * HEAD_DIM), 1.0, 6.0, ((0, 8), (2, 4))),
        "z_pre": centred(streams_of[3], (NUM_STREAMS, SEQ_LEN, HEADS * HEAD_DIM), 1.0, 6.0, ((0, 8), (2, 4))),
        "b_pre": centred(streams_of[4], (NUM_STREAMS, SEQ_LEN, GROUPS * STATE), 1.0, 6.0, ((0, 8),)),
        "c_pre": centred(streams_of[5], (NUM_STREAMS, SEQ_LEN, GROUPS * STATE), 1.0, 6.0, ((0, 8),)),
        "dt_raw": draw_dt_raw(jax.random.fold_in(streams_of[14], 71), 0),
        "conv_x": centred(streams_of[7], (CONV, HEADS * HEAD_DIM), CONV ** -0.5, 3.0, ((1, 4),)),
        "conv_b": centred(streams_of[8], (CONV, GROUPS * STATE), CONV ** -0.5, 3.0),
        "conv_c": centred(streams_of[9], (CONV, GROUPS * STATE), CONV ** -0.5, 3.0),
        "dt_bias": jnp.clip(-3.8 + 0.5999999 * jax.random.uniform(streams_of[10], (HEADS,), jnp.float32) ** level_of(streams_of[10], (HEADS,), ((0, 4),), -0.2, 0.2), -3.8, -3.2),
        "a_log": draw_a_log(jax.random.fold_in(streams_of[14], 71), 0),
        "d_skip": jnp.clip(0.5 + 1.0 * jax.random.uniform(streams_of[12], (HEADS,), jnp.float32) ** level_of(streams_of[12], (HEADS,), ((0, 4),), -0.2, 0.2), 0.5, 1.5),
        "norm_w": jnp.clip(1.0 + 0.18 * jax.random.normal(streams_of[13], (HEADS * HEAD_DIM,), jnp.float32), 0.1, 1.9),
    }


def causal_filter(signal, taps):
    tap_count = taps.shape[0]
    overall_span_tokens = signal.shape[1]
    padded = jnp.pad(signal, ((0, 0), (tap_count - 1, 0), (0, 0)))
    filtered = padded[:, 0:overall_span_tokens] * taps[0]
    for offset in range(1, tap_count):
        filtered = filtered + padded[:, offset:offset + overall_span_tokens] * taps[offset]
    return filtered

def mixer_out(x_input, state_source_vector, c_input, z_input, rate_raw, rate_log, x_filter, b_filter, readout_filter, rate_bias, skip_gain, norm_gain, block_len):
    highest = lax.Precision.HIGHEST
    seqs_here, overall_span_tokens, channels = x_input.shape
    head_count = rate_raw.shape[2]
    head_size = channels // head_count
    blocks = overall_span_tokens // block_len
    x_act = jax.nn.silu(causal_filter(x_input, x_filter))
    b_act = jax.nn.silu(causal_filter(state_source_vector, b_filter))
    c_act = jax.nn.silu(causal_filter(c_input, readout_filter))
    step_rate = jax.nn.softplus(rate_raw + rate_bias)
    log_step = -step_rate * jnp.exp(rate_log)
    x_heads = x_act.reshape(seqs_here, overall_span_tokens, head_count, head_size)
    scaled = (x_heads * step_rate[..., None]).reshape(seqs_here, blocks, block_len, head_count, head_size)
    b_blocks = b_act.reshape(seqs_here, blocks, block_len, -1)
    c_blocks = c_act.reshape(seqs_here, blocks, block_len, -1)
    cum_log = jnp.cumsum(jnp.swapaxes(log_step, 1, 2).reshape(seqs_here, head_count, blocks, block_len), axis=3)
    causal = jnp.tril(jnp.ones((block_len, block_len), dtype=bool))[None, None, None]
    spread = cum_log[..., :, None] - cum_log[..., None, :]
    decays = jnp.exp(jnp.where(causal, spread, -jnp.inf))
    scores = jnp.einsum('abln,absn->abls', c_blocks, b_blocks, precision=highest)
    within = jnp.einsum('arbls,absrp->ablrp', scores[:, None] * decays, scaled, precision=highest)
    to_end = jnp.transpose(jnp.exp(cum_log[..., -1:] - cum_log), (0, 2, 3, 1))
    pieces = jnp.einsum('absn,absrp->abrpn', b_blocks, scaled * to_end[..., None], precision=highest)
    block_fades = jnp.moveaxis(jnp.exp(cum_log[..., -1]), 2, 0)

    def carry_step(carried, inputs):
        addend, factor = inputs
        return (carried * factor[:, :, None, None] + addend, carried)
    initial = jnp.zeros((seqs_here, head_count, head_size, b_blocks.shape[-1]), jnp.float32)
    _, entering = lax.scan(carry_step, initial, (jnp.moveaxis(pieces, 1, 0), block_fades))
    entering = jnp.moveaxis(entering, 0, 1)
    from_start = jnp.transpose(jnp.exp(cum_log), (0, 2, 3, 1))
    carried_in = jnp.einsum('abln,abrpn->ablrp', c_blocks, entering, precision=highest) * from_start[..., None]
    mixed = (within + carried_in).reshape(seqs_here, overall_span_tokens, head_count, head_size) + skip_gain[:, None] * x_heads
    gated = mixed * jax.nn.silu(z_input.reshape(seqs_here, overall_span_tokens, head_count, head_size))
    inverse_rms = lax.rsqrt(lax.optimization_barrier(jnp.mean(gated * gated, axis=-1, keepdims=True)) + 1e-05)
    return (gated * inverse_rms * norm_gain.reshape(head_count, head_size)).reshape(seqs_here, overall_span_tokens, channels)

def reference(cotangent, layer_input, x_pre, z_pre, b_pre, c_pre, dt_raw, conv_x, conv_b, conv_c, dt_bias, a_log, d_skip, norm_w):
    runs = N_SP
    run_heads = HEADS // runs
    run_width = run_heads * HEAD_DIM
    group_span = runs // GROUPS
    overall_span_tokens = x_pre.shape[1]

    def by_run(values, each_width):
        return jnp.transpose(values.reshape(1, overall_span_tokens, runs, each_width), (2, 0, 1, 3))

    def by_group(values):
        repeated = jnp.repeat(values.reshape(1, overall_span_tokens, GROUPS, STATE), group_span, axis=2)
        return jnp.transpose(repeated, (2, 0, 1, 3))

    def back_tokens(values):
        return jnp.transpose(values, (1, 2, 0, 3)).reshape(overall_span_tokens, -1)
    x_taps = jnp.transpose(conv_x.astype(jnp.float32).reshape(CONV, runs, run_width), (1, 0, 2))
    b_taps = jnp.transpose(jnp.repeat(conv_b.astype(jnp.float32).reshape(CONV, GROUPS, STATE), group_span, axis=1), (1, 0, 2))
    c_taps = jnp.transpose(jnp.repeat(conv_c.astype(jnp.float32).reshape(CONV, GROUPS, STATE), group_span, axis=1), (1, 0, 2))
    bias_runs = dt_bias.reshape(runs, run_heads)
    log_runs = a_log.reshape(runs, run_heads)
    skip_runs = d_skip.reshape(runs, run_heads)
    gain_runs = norm_w.reshape(runs, run_width)

    def single_pass(x_in, b_in, c_in, z_in, rate_in, log_in, x_tap, b_tap, c_tap, bias_in, skip_in, gain_in, cot_in):

        def forward(x_input, state_source_vector, c_input, z_input, rate_raw, rate_log):
            return mixer_out(x_input, state_source_vector, c_input, z_input, rate_raw, rate_log, x_tap, b_tap, c_tap, bias_in, skip_in, gain_in, BLOCK)
        _, pullback = jax.vjp(forward, x_in, b_in, c_in, z_in, rate_in, log_in)
        return pullback(cot_in)

    def group_sum(partial_value):
        rounded = lax.optimization_barrier(partial_value.astype(jnp.bfloat16)).astype(jnp.float32)
        summed = lax.optimization_barrier(jnp.sum(rounded.reshape(GROUPS, group_span, overall_span_tokens, STATE), axis=1))
        return jnp.transpose(summed, (1, 0, 2)).reshape(overall_span_tokens, GROUPS * STATE).astype(jnp.bfloat16)

    def per_sequence(items):
        cot_seq, x_seq, z_seq, b_seq, c_seq, rate_seq = items
        gradients = jax.vmap(single_pass)(by_run(x_seq.astype(jnp.float32), run_width), by_group(b_seq.astype(jnp.float32)), by_group(c_seq.astype(jnp.float32)), by_run(z_seq.astype(jnp.float32), run_width), by_run(rate_seq.astype(jnp.float32), run_heads), log_runs, x_taps, b_taps, c_taps, bias_runs, skip_runs, gain_runs, by_run(cot_seq.astype(jnp.float32), run_width))
        grad_x, grad_b, grad_c, grad_z, grad_rate, grad_log = gradients
        return (back_tokens(grad_x).astype(jnp.bfloat16), back_tokens(grad_z).astype(jnp.bfloat16), group_sum(grad_b), group_sum(grad_c), back_tokens(grad_rate).astype(jnp.bfloat16), grad_log.reshape(HEADS))
    d_x_pre, d_z_pre, d_b_pre, d_c_pre, d_dt_raw, log_parts = lax.map(per_sequence, (cotangent, x_pre, z_pre, b_pre, c_pre, dt_raw))
    grad_a_log = lax.optimization_barrier(jnp.sum(log_parts, axis=0))
    grad_w_dt = jnp.dot(layer_input.reshape(-1, D).T, d_dt_raw.reshape(-1, HEADS), preferred_element_type=jnp.float32)
    return (d_x_pre, d_z_pre, d_b_pre, d_c_pre, d_dt_raw, grad_a_log, grad_w_dt)
```

```python
import functools

import jax
import jax.numpy as jnp
from jax import lax
from jax.experimental import pallas as pl
from jax.experimental.pallas import tpu as pltpu
from jax.sharding import PartitionSpec as P

GROUPS = 2
STATE = 128
BLOCK = 128
LANES = 128
ROWS = 8
PAD = 8
CUT = 1
WAVE = 4
EPS = 1e-05
LOG2E = 1.4426950408889634
MESH = pl.DeviceIdType.MESH
F32 = jnp.float32
BF16 = jnp.bfloat16
ROWS_ROWS = ((1,), (1,))
COLS_COLS = ((0,), (0,))


def dot(a, b, dims=((1,), (0,)), precision=None):
    return lax.dot_general(a, b, (dims, ((), ())), precision=precision, preferred_element_type=F32)


def iota(axis, shape=(BLOCK, LANES)):
    return lax.broadcasted_iota(jnp.int32, shape, axis)


def silu_parts(u):
    sig = jax.nn.sigmoid(u)
    act = u * sig
    return act, sig + act * (1.0 - sig)


def halves(v):
    hi = v.astype(BF16)
    return jnp.concatenate([hi, (v - hi.astype(F32)).astype(BF16)], axis=1)


def add_all(parts):
    return functools.reduce(lambda a, b: a + b, parts)


def step_kernel(
    n_sp,
    n_dp,
    group_span,
    head_dim,
    heads,
    reduce_here,
    cot_hbm,
    li_hbm,
    x_hbm,
    z_hbm,
    b_hbm,
    c_hbm,
    dt_hbm,
    tapx_hbm,
    tapb_hbm,
    tapc_hbm,
    bias_hbm,
    alog_hbm,
    skip_hbm,
    nw_hbm,
    ox_ref,
    oz_ref,
    ob_ref,
    oc_ref,
    od_ref,
    oga_ref,
    ow_ref,
    cot_v,
    li_v,
    x_v,
    z_v,
    b_v,
    c_v,
    dt_v,
    tapx_v,
    tapb_v,
    tapc_v,
    bias_v,
    alog_v,
    skip_v,
    nw_v,
    cotr_s,
    xf_s,
    bf_s,
    cf_s,
    xa_s,
    gx_s,
    y_s,
    dtp_s,
    ea_s,
    te_s,
    sin_s,
    ds_s,
    st_s,
    lam_s,
    m_s,
    xdb_s,
    xdte_s,
    dy_s,
    edy_s,
    du_s,
    bb_s,
    cb_s,
    gb_s,
    gc_s,
    ct_s,
    dbu_s,
    dcu_s,
    cp_s,
    dtt_s,
    step_s,
    cum_s,
    sig_s,
    ga_s,
    acc_s,
    dyf_s,
    dsf_s,
    dz_s,
    dx_s,
    dbc_s,
    dd_s,
    rbc,
    rd,
    rga,
    part,
    rs1,
    mine1,
    rs2,
    mine2,
    rs3,
    in_sem,
    cot_send,
    cot_recv,
    z_send,
    z_recv,
    x_send,
    x_recv,
    bc_send,
    bc_recv,
    d_send,
    d_recv,
    ga_send,
    ga_recv,
    w1_send,
    w1_recv,
    w2_send,
    w2_recv,
    w3_send,
    w3_recv,
):
    pairs, length, _ = x_v.shape
    channels = pairs * LANES
    tokens = oz_ref.shape[0]
    chunks = length // BLOCK
    per = LANES // head_dim
    sp = lax.axis_index("sp")
    dp = lax.axis_index("dp")
    sp_peers = [lax.rem(sp + o, n_sp) for o in range(1, n_sp)]
    dp_peers = [lax.rem(dp + o, n_dp) for o in range(1, n_dp)] if reduce_here else []
    gcol = pl.multiple_of((sp // group_span) * STATE, STATE)
    gcols = pl.ds(gcol, STATE)

    def block(c, size=BLOCK):
        return pl.ds(pl.multiple_of(c * size, size), size)

    ours = block(sp, tokens)

    loads = {}

    def load(name, src, dst):
        loads[name] = loads.get(name, []) + [pltpu.make_async_copy(src, dst, in_sem.at[sum(map(len, loads.values()))])]
        loads[name][-1].start()

    def arrived(*names):
        for name in names:
            for copy in loads[name]:
                copy.wait()

    load("dt", dt_hbm, dt_v)
    load("dt", bias_hbm, bias_v)
    load("dt", alog_hbm, alog_v)
    load("bc", b_hbm.at[:, gcols], b_v)
    load("bc", c_hbm.at[:, gcols], c_v)
    load("bc", tapb_hbm, tapb_v)
    load("bc", tapc_hbm, tapc_v)
    load("x", tapx_hbm, tapx_v)
    load("x", skip_hbm, skip_v)
    load("x", nw_hbm, nw_v)
    for j in range(pairs):
        load("x", x_hbm.at[:, pl.ds(j * LANES, LANES)], x_v.at[j])
    load("cot", cot_hbm, cot_v)
    for j in range(pairs):
        load("z", z_hbm.at[:, pl.ds(j * LANES, LANES)], z_v.at[j])
    load("li", li_hbm, li_v)

    barrier = pltpu.get_barrier_semaphore()
    for peer in sp_peers:
        pl.semaphore_signal(barrier, inc=1, device_id={"sp": peer}, device_id_type=MESH)
    for peer in dp_peers:
        pl.semaphore_signal(barrier, inc=1, device_id={"dp": peer}, device_id_type=MESH)

    def remote(src, dst, send, recv, axis, peer):
        return pltpu.make_async_remote_copy(
            src_ref=src, dst_ref=dst, send_sem=send, recv_sem=recv,
            device_id={axis: peer}, device_id_type=MESH,
        )

    def cot_copy(peer, recv, j):
        return remote(
            cot_v.at[:, block(peer * pairs + j, LANES)], cotr_s.at[j, block(recv, tokens)],
            cot_send.at[peer, j], cot_recv.at[recv, j], "sp", peer,
        )

    def z_copy(peer, recv, j):
        return remote(
            dz_s.at[j, block(peer, tokens)], oz_ref.at[:, block(recv * pairs + j, LANES)],
            z_send.at[peer, j], z_recv.at[recv, j], "sp", peer,
        )

    def x_copy(peer, recv, j):
        return remote(
            dx_s.at[j, block(peer, tokens)], ox_ref.at[:, block(recv * pairs + j, LANES)],
            x_send.at[peer, j], x_recv.at[recv, j], "sp", peer,
        )

    def bc_copy(peer, recv):
        return remote(
            dbc_s.at[block(peer, tokens)], rbc.at[recv], bc_send.at[peer], bc_recv.at[recv], "sp", peer,
        )

    def d_copy(peer, recv):
        return remote(dd_s.at[peer], rd.at[recv], d_send.at[peer], d_recv.at[recv], "sp", peer)

    lane = iota(1)
    row = iota(0)
    half = [lane // head_dim == k for k in range(per)]
    half_b = [jnp.where(iota(1, (1, LANES)) // head_dim == k, 1.0, 0.0).astype(BF16) for k in range(per)]
    causal = row >= lane
    tri = jnp.where(causal, 1.0, 0.0).astype(BF16)
    same = jnp.where(row // head_dim == lane // head_dim, 1.0 / head_dim, 0.0).astype(BF16)
    same = jnp.concatenate([same, same], axis=0)

    def pick(parts):
        out = parts[-1]
        for k in range(per - 1):
            out = jnp.where(half[k][: out.shape[0]], parts[k], out)
        return out

    def column(v):
        v = v[...]
        n = v.shape[1]
        diag = iota(0, (ROWS, n)) == iota(1, (ROWS, n))
        return jnp.sum(jnp.where(diag, jnp.broadcast_to(v, (ROWS, n)), 0.0), axis=1, keepdims=True)

    arrived("dt")
    decay = jnp.exp(column(alog_v))
    raw = dt_v[...].astype(F32)
    if heads < ROWS:
        raw = jnp.concatenate([raw, jnp.zeros((ROWS - heads, length), F32)], axis=0)
    pre = raw + column(bias_v)
    live = iota(0, (ROWS, length)) < heads
    dt = jnp.where(live, jnp.maximum(pre, 0.0) + jnp.log1p(jnp.exp(-jnp.abs(pre))), 0.0)
    dtt_s[...] = dt
    step_s[...] = -dt * decay
    sig_s[...] = jax.nn.sigmoid(pre)
    log_step = dt * (-LOG2E * decay)
    log_step = jnp.concatenate([log_step[:, c * BLOCK : (c + 1) * BLOCK] for c in range(chunks)], axis=0)
    first = log_step.astype(BF16)
    rest = log_step - first.astype(F32)
    triu = jnp.where(row <= lane, 1.0, 0.0).astype(BF16)
    cum_s[...] = dot(
        jnp.concatenate([first, halves(rest)], axis=1), jnp.concatenate([triu, triu, triu], axis=0)
    )
    arrived("bc", "x")

    cp_s[0:1, :] = nw_v[...]
    skip = skip_v[...]
    for j in range(pairs):
        cp_s[1:2, j * LANES : (j + 1) * LANES] = pick(
            [jnp.broadcast_to(skip[0:1, j * per + k : j * per + k + 1], (1, LANES)) for k in range(per)]
        )

    zeros8 = jnp.zeros((PAD, LANES), F32)
    bf_s[0:PAD, :] = zeros8
    cf_s[0:PAD, :] = zeros8
    dbu_s[length : length + PAD, :] = zeros8
    dcu_s[length : length + PAD, :] = zeros8
    for j in range(pairs):
        xf_s[j, 0:PAD, :] = zeros8
        du_s[j, length : length + PAD, :] = zeros8
    st_s[...] = jnp.zeros_like(st_s)

    def conv(ref, base, taps):
        n = taps.shape[0]
        return add_all(
            [ref[pl.ds(base + (PAD - (n - 1 - k)), BLOCK), :] * taps[k : k + 1] for k in range(n)]
        )

    def conv_back(ref, base, taps):
        n = taps.shape[0]
        return add_all([ref[pl.ds(base + (n - 1 - k), BLOCK), :] * taps[k : k + 1] for k in range(n)])

    def forward(c, carry):
        @pl.when(c == min(CUT, chunks - 1))
        def _():
            pl.semaphore_wait(barrier, len(sp_peers) + len(dp_peers))
            arrived("cot")
            for j in range(pairs):
                for peer in sp_peers:
                    cot_copy(peer, sp, j).start()

        base = pl.multiple_of(c * BLOCK, BLOCK)
        rows = pl.ds(base, BLOCK)
        padded = pl.ds(base + PAD, BLOCK)
        bf_s[padded, :] = b_v[rows, :].astype(F32)
        cf_s[padded, :] = c_v[rows, :].astype(F32)
        for j in range(pairs):
            xf_s[j, padded, :] = x_v[j, rows, :].astype(F32)
        ba, gb = silu_parts(conv(bf_s, base, tapb_v[:, gcols].astype(F32)))
        ca, gc = silu_parts(conv(cf_s, base, tapc_v[:, gcols].astype(F32)))
        gb_s[rows, :] = gb
        gc_s[rows, :] = gc
        bb = ba.astype(BF16)
        cb = ca.astype(BF16)
        bb_s[rows, :] = bb
        cb_s[rows, :] = cb
        ct_s[rows, :] = ca.T.astype(BF16)
        b2 = halves(ba)
        c2 = halves(ca)
        c3 = jnp.concatenate([c2, cb], axis=1)
        scores = dot(c3, jnp.concatenate([bb, bb, b2[:, STATE:]], axis=1), ROWS_ROWS)
        bt2 = halves(ba.T)
        dt_c = dtt_s[:, rows]
        cum = cum_s[pl.ds(pl.multiple_of(c * ROWS, ROWS), ROWS), :]
        cols_t = jnp.concatenate([cum, dt_c, jnp.zeros((LANES - 2 * ROWS, LANES), F32)], axis=0).T
        for j in range(pairs):
            cols = pl.ds(j * LANES, LANES)
            xa, gx = silu_parts(conv(xf_s.at[j], base, tapx_v[:, cols].astype(F32)))
            gx_s[j, rows, :] = gx
            xa_s[j, rows, :] = xa
            acols, dcols, his, los = [], [], [], []
            for k in range(per):
                h = j * per + k
                acol = jnp.broadcast_to(cols_t[:, h : h + 1], (BLOCK, LANES))
                acols.append(acol)
                dcols.append(jnp.broadcast_to(cols_t[:, ROWS + h : ROWS + h + 1], (BLOCK, LANES)))
                lam = jnp.exp2(jnp.where(causal, acol - cum[h : h + 1, :], -jnp.inf))
                m = scores * lam
                hi = m.astype(BF16)
                his.append(hi)
                los.append((m - hi.astype(F32)).astype(BF16))
                lam_s[j, rows, k * BLOCK : (k + 1) * BLOCK] = lam
                m_s[j, rows, k * BLOCK : (k + 1) * BLOCK] = hi
            ap = pick(acols)
            dtp = pick(dcols)
            dtp_s[j, rows, :] = dtp
            ea = jnp.exp2(ap)
            te = jnp.exp2(ap[BLOCK - 1 : BLOCK, :] - ap)
            ea_s[j, rows, :] = ea
            te_s[j, rows, :] = te
            xd = xa * dtp
            xd_hi = xd.astype(BF16)
            xd_lo = (xd - xd_hi.astype(F32)).astype(BF16)
            xdte = (xd * te).astype(BF16)
            xdb_s[j, rows, :] = xd_hi
            xdte_s[j, rows, :] = xdte
            cat_hi = [xd_hi * h for h in half_b]
            y = dot(
                jnp.concatenate(his + los + his, axis=1),
                jnp.concatenate(cat_hi + cat_hi + [xd_lo * h for h in half_b], axis=0),
            )
            st = st_s[j]
            sin_s[j, rows, :] = st
            st_hi = st.astype(BF16)
            st_lo = (st - st_hi.astype(F32)).astype(BF16)
            y_s[j, rows, :] = y + dot(c3, jnp.concatenate([st_hi, st_hi, st_lo], axis=0)) * ea
            st_s[j] = st * ea[BLOCK - 1 : BLOCK, :] + dot(bt2, jnp.concatenate([xdte, xdte], axis=0))
        return carry

    lax.fori_loop(0, chunks, forward, 0)

    for j in range(pairs):
        cotr_s[j, ours, :] = cot_v[:, block(sp * pairs + j, LANES)]
    arrived("z")
    acc_s[...] = jnp.zeros_like(acc_s)

    def middle(j, carry):
        cols = block(j, LANES)
        for peer in sp_peers:
            cot_copy(peer, peer, j).wait_recv()
        gain = cp_s[0:1, cols]
        skips = cp_s[1:2, cols]
        place_r = jnp.where(row // head_dim + j * per == lane, 1.0, 0.0).astype(BF16)
        place_q = jnp.where(row // head_dim + (j * per + LANES // 2) == lane, 1.0, 0.0).astype(BF16)
        place_r = jnp.concatenate([place_r, place_r], axis=0)
        for start in range(0, chunks, WAVE):
            wave = list(reversed(range(chunks)))[start : start + WAVE]
            state = []
            for c in wave:
                rows = pl.ds(c * BLOCK, BLOCK)
                full = y_s[j, rows, :] + skips * xa_s[j, rows, :]
                sz, gz = silu_parts(z_v[j, rows, :].astype(F32))
                gated = full * sz
                state.append((full, sz, gz, gated, dot(halves(gated * gated), same)))
            means = []
            for c, (full, sz, gz, gated, power) in zip(wave, state):
                inv = lax.rsqrt(power + EPS)
                gh = gated * inv
                g = cotr_s[j, pl.ds(c * BLOCK, BLOCK), :].astype(F32) * gain
                means.append((inv, gh, g, dot(halves(g * gh), same)))
            for c, (full, sz, gz, gated, _), (inv, gh, g, mean) in zip(wave, state, means):
                rows = pl.ds(c * BLOCK, BLOCK)
                dgated = inv * (g - gh * mean)
                dz_s[j, rows, :] = (dgated * full * gz).astype(BF16)
                dy = dgated * sz
                dyf_s[rows, :] = dy
                dy_s[j, rows, :] = halves(dy)
                edy_s[j, rows, :] = (ea_s[j, rows, :] * dy).astype(BF16)
        ds = jnp.zeros((STATE, LANES), F32)
        for c in reversed(range(chunks)):
            rows = pl.ds(c * BLOCK, BLOCK)
            dsf_s[rows, :] = ds
            ds_s[j, rows, :] = ds.astype(BF16)
            if c > 0:
                last = pl.ds(c * BLOCK + BLOCK - 1, 1)
                ds = ds * ea_s[j, last, :] + dot(ct_s[rows, :], edy_s[j, rows, :])
        for c in reversed(range(chunks)):
            rows = pl.ds(c * BLOCK, BLOCK)
            dy2 = dy_s[j, rows, :]
            mt = jnp.concatenate(
                [m_s[j, rows, k * BLOCK : (k + 1) * BLOCK].astype(F32).T.astype(BF16) for k in range(per)], axis=1
            )
            dycat = [dy2[:, p * LANES : (p + 1) * LANES] * h for p in range(2) for h in half_b]
            dstate = te_s[j, rows, :] * dot(bb_s[rows, :], ds_s[j, rows, :])
            dxd = dot(jnp.concatenate([mt, mt], axis=1), jnp.concatenate(dycat, axis=0)) + dstate
            xa = xa_s[j, rows, :]
            dtp = dtp_s[j, rows, :]
            dy = dyf_s[rows, :]
            tail = jnp.sum(xa * dtp * dstate, axis=0, keepdims=True) + ea_s[
                j, pl.ds(c * BLOCK + BLOCK - 1, 1), :
            ] * jnp.sum(dsf_s[rows, :] * sin_s[j, rows, :], axis=0, keepdims=True)
            q = dxd * xa
            r = dy * y_s[j, rows, :] - q * dtp
            r = jnp.concatenate(
                [
                    r[: BLOCK - ROWS],
                    r[BLOCK - ROWS :] + jnp.where(iota(0, (ROWS, LANES)) == ROWS - 1, tail, 0.0),
                ],
                axis=0,
            )
            acc_s[rows, :] = acc_s[rows, :] + dot(halves(r), place_r) + dot(q.astype(BF16), place_q)
            du_s[j, rows, :] = (dxd * dtp + skips * dy) * gx_s[j, rows, :]
        for peer in sp_peers:
            z_copy(peer, sp, j).start()
        return carry

    lax.fori_loop(0, pairs, middle, 0)

    acc_t = [acc_s[pl.ds(c * BLOCK, BLOCK), :].T for c in range(chunks)]
    dlogs = dot(
        halves(jnp.concatenate([t[0:ROWS] for t in acc_t], axis=0)), jnp.concatenate([tri, tri], axis=0)
    )
    ga = jnp.zeros((ROWS, LANES), F32)
    for c in range(chunks):
        rows = pl.ds(c * BLOCK, BLOCK)
        dlog = dlogs[c * ROWS : (c + 1) * ROWS]
        ddt = acc_t[c][LANES // 2 : LANES // 2 + ROWS] - dlog * decay
        dd_s[c] = (ddt * sig_s[:, rows]).astype(BF16)
        ga = ga + dlog * step_s[:, rows]
    for peer in sp_peers:
        d_copy(peer, sp).start()
    ga_col = jnp.sum(ga, axis=1, keepdims=True)

    def ga_row(col):
        diag = iota(0, (ROWS, heads)) == iota(1, (ROWS, heads))
        return jnp.sum(jnp.where(diag, jnp.broadcast_to(col, (ROWS, heads)), 0.0), axis=0, keepdims=True)

    def ga_copy(peer, recv):
        return remote(ga_s, rga.at[recv], ga_send.at[peer], ga_recv.at[recv], "dp", peer)

    if reduce_here:
        ga_s[...] = jnp.broadcast_to(ga_col, ga_s.shape)
        for peer in dp_peers:
            ga_copy(peer, dp).start()
    else:
        oga_ref[...] = ga_row(ga_col)

    def convolve(i, carry):
        c = chunks - 1 - i
        base = pl.multiple_of(c * BLOCK, BLOCK)
        rows = pl.ds(base, BLOCK)
        for j in range(pairs):
            cols = pl.ds(j * LANES, LANES)
            dx_s[j, rows, :] = conv_back(du_s.at[j], base, tapx_v[:, cols].astype(F32)).astype(BF16)
        return carry

    lax.fori_loop(0, chunks, convolve, 0)
    for j in range(pairs):
        for peer in sp_peers:
            x_copy(peer, sp, j).start()

    def backward(i, carry):
        c = chunks - 1 - i
        base = pl.multiple_of(c * BLOCK, BLOCK)
        rows = pl.ds(base, BLOCK)
        dscores = jnp.zeros((BLOCK, BLOCK), F32)
        dcc = jnp.zeros((BLOCK, STATE), F32)
        dbb = jnp.zeros((BLOCK, STATE), F32)
        for j in range(pairs):
            cols = pl.ds(j * LANES, LANES)
            xdb = xdb_s[j, rows, :]
            xcat = jnp.concatenate([xdb * h for h in half_b], axis=0)
            dm = dot(dy_s[j, rows, :], jnp.concatenate([xcat, xcat], axis=1), ROWS_ROWS) * lam_s[j, rows, :]
            for k in range(per):
                dscores = dscores + dm[:, k * BLOCK : (k + 1) * BLOCK]

        def joined(ref):
            return jnp.concatenate([ref[j, rows, :].astype(BF16) for j in range(pairs)], axis=1)

        dcc = dot(joined(edy_s), joined(sin_s), ROWS_ROWS)
        dbb = dot(joined(xdte_s), joined(ds_s), ROWS_ROWS)
        dcc = dcc + dot(dscores.astype(BF16), bb_s[rows, :])
        dbb = dbb + dot(dscores.T.astype(BF16), cb_s[rows, :])
        dbu_s[rows, :] = dbb * gb_s[rows, :]
        dcu_s[rows, :] = dcc * gc_s[rows, :]
        dbc_s[rows, 0:STATE] = conv_back(dbu_s, base, tapb_v[:, gcols].astype(F32)).astype(BF16)
        dbc_s[rows, STATE : 2 * STATE] = conv_back(dcu_s, base, tapc_v[:, gcols].astype(F32)).astype(BF16)
        return carry

    mid = chunks // 2
    lax.fori_loop(0, mid, backward, 0)

    rd[sp] = dd_s[sp]
    for peer in sp_peers:
        d_copy(peer, peer).wait_recv()
    whole_d = jnp.concatenate([rd[k].astype(F32)[:heads] for k in range(n_sp)], axis=0).astype(BF16)
    od_ref[...] = whole_d
    arrived("li")
    whole_w = dot(whole_d, li_v[...])

    if reduce_here:
        width = part.shape[1] // n_dp

        def w1_copy(peer, recv):
            return remote(
                part.at[:, block(peer, width)], rs1.at[recv], w1_send.at[peer], w1_recv.at[recv], "dp", peer
            )

        def w2_copy(peer, recv):
            return remote(mine1, rs2.at[recv], w2_send.at[peer], w2_recv.at[recv], "sp", peer)

        def w3_copy(peer, recv):
            return remote(mine2, rs3.at[recv], w3_send.at[peer], w3_recv.at[recv], "dp", peer)

        part[...] = whole_w.astype(BF16)
        for peer in dp_peers:
            w1_copy(peer, dp).start()
        rs1[dp] = part[:, block(dp, width)]
    else:
        ow_ref[...] = whole_w

    lax.fori_loop(mid, chunks, backward, 0)

    if reduce_here:
        for peer in dp_peers:
            w1_copy(peer, peer).wait_recv()
        mine1[...] = add_all([rs1[k].astype(F32) for k in range(n_dp)]).astype(BF16)
        for peer in sp_peers:
            w2_copy(peer, sp).start()
        for peer in sp_peers:
            bc_copy(peer, sp).start()
        rs2[sp] = mine1[...]
        rga[dp] = ga_s[...]
        for peer in dp_peers:
            ga_copy(peer, peer).wait_recv()
        oga_ref[...] = ga_row(add_all([rga[k] for k in range(n_dp)])[:, 0:1])
        for peer in sp_peers:
            w2_copy(peer, peer).wait_recv()
        mine2[...] = add_all([rs2[k].astype(F32) for k in range(n_sp)]).astype(BF16)
        for peer in dp_peers:
            w3_copy(peer, dp).start()
        rs3[dp] = mine2[...]

    else:
        for peer in sp_peers:
            bc_copy(peer, sp).start()
    for j in range(pairs):
        oz_ref[:, block(sp * pairs + j, LANES)] = dz_s[j, ours, :]
        ox_ref[:, block(sp * pairs + j, LANES)] = dx_s[j, ours, :]
    rbc[sp] = dbc_s[ours, :]
    for peer in sp_peers:
        bc_copy(peer, peer).wait_recv()
    for g in range(GROUPS):
        total = add_all([rbc[g * group_span + k].astype(F32) for k in range(group_span)]).astype(BF16)
        ob_ref[:, g * STATE : (g + 1) * STATE] = total[:, 0:STATE]
        oc_ref[:, g * STATE : (g + 1) * STATE] = total[:, STATE : 2 * STATE]
    for peer in sp_peers:
        for j in range(pairs):
            z_copy(peer, peer, j).wait_recv()
            x_copy(peer, peer, j).wait_recv()
    if reduce_here:
        for peer in dp_peers:
            w3_copy(peer, peer).wait_recv()
        for k in range(n_dp):
            ow_ref[:, k * width : (k + 1) * width] = rs3[k].astype(F32)
    for peer in sp_peers:
        for copy in (bc_copy, d_copy):
            copy(peer, sp).wait_send()
        for j in range(pairs):
            cot_copy(peer, sp, j).wait_send()
            z_copy(peer, sp, j).wait_send()
            x_copy(peer, sp, j).wait_send()
        if reduce_here:
            w2_copy(peer, sp).wait_send()
    for peer in dp_peers:
        for copy in (ga_copy, w1_copy, w3_copy):
            copy(peer, dp).wait_send()


def fused(args, n_sp, n_dp, group_span, head_dim, heads, reduce_here):
    cot, li, x, z, b, c, dt, tapx, tapb, tapc, bias, alog, skip, nw = args
    length, channels = x.shape
    tokens, width = li.shape
    all_heads = heads * n_sp
    per = LANES // head_dim
    pairs = channels // LANES
    vm = pltpu.VMEM
    dma = pltpu.SemaphoreType.DMA
    wide = vm((pairs, length, LANES), F32)
    wide_b = vm((pairs, length, LANES), BF16)
    thin = vm((length, LANES), F32)
    thin_b = vm((length, LANES), BF16)
    padded = vm((length + PAD, LANES), F32)
    tall = vm((pairs, length + PAD, LANES), F32)
    rows = vm((ROWS, length), F32)
    piece = width // n_dp if reduce_here else LANES
    return pl.pallas_call(
        functools.partial(step_kernel, n_sp, n_dp, group_span, head_dim, heads, reduce_here),
        out_shape=(
            jax.ShapeDtypeStruct((tokens, channels * n_sp), BF16),
            jax.ShapeDtypeStruct((tokens, channels * n_sp), BF16),
            jax.ShapeDtypeStruct((tokens, GROUPS * STATE), BF16),
            jax.ShapeDtypeStruct((tokens, GROUPS * STATE), BF16),
            jax.ShapeDtypeStruct((all_heads, tokens), BF16),
            jax.ShapeDtypeStruct((1, heads), F32),
            jax.ShapeDtypeStruct((all_heads, width), F32),
        ),
        in_specs=[pl.BlockSpec(memory_space=pltpu.MemorySpace.HBM)] * 14,
        out_specs=tuple([pl.BlockSpec(memory_space=pltpu.VMEM)] * 7),
        scratch_shapes=[
            vm((tokens, channels * n_sp), BF16),
            vm((tokens, width), BF16),
            wide_b,
            wide_b,
            thin_b,
            thin_b,
            vm((heads, length), BF16),
            vm(tapx.shape, BF16),
            vm(tapb.shape, BF16),
            vm(tapc.shape, BF16),
            vm((1, heads), F32),
            vm((1, heads), F32),
            vm((1, heads), F32),
            vm((1, channels), F32),
            wide_b,
            tall,
            padded,
            padded,
            wide,
            wide,
            wide,
            wide,
            wide,
            wide,
            wide,
            wide_b,
            vm((pairs, STATE, LANES), F32),
            vm((pairs, length, per * BLOCK), F32),
            vm((pairs, length, per * BLOCK), BF16),
            wide_b,
            wide_b,
            vm((pairs, length, 2 * LANES), BF16),
            wide_b,
            tall,
            thin_b,
            thin_b,
            thin,
            thin,
            thin_b,
            padded,
            padded,
            vm((ROWS, channels), F32),
            rows,
            rows,
            vm((length // BLOCK * ROWS, LANES), F32),
            rows,
            vm((ROWS, LANES), F32),
            thin,
            thin,
            thin,
            wide_b,
            wide_b,
            vm((length, 2 * STATE), BF16),
            vm((length // BLOCK, ROWS, BLOCK), BF16),
            vm((n_sp, tokens, 2 * STATE), BF16),
            vm((n_sp, ROWS, BLOCK), BF16),
            vm((n_dp, ROWS, LANES), F32),
            vm((all_heads, width), BF16),
            vm((n_dp, all_heads, piece), BF16),
            vm((all_heads, piece), BF16),
            vm((n_sp, all_heads, piece), BF16),
            vm((all_heads, piece), BF16),
            vm((n_dp, all_heads, piece), BF16),
            dma((12 + 2 * pairs,)),
        ]
        + [dma((n_sp, pairs))] * 6
        + [dma((n_sp,))] * 4
        + [dma((n_dp,))] * 4
        + [dma((n_sp,))] * 2
        + [dma((n_dp,))] * 2,
        compiler_params=pltpu.CompilerParams(
            collective_id=0, has_side_effects=True, vmem_limit_bytes=40 * 1024 * 1024
        ),
    )(*args)


def out_kernel(count, *refs):
    srcs, dsts, sem = refs[:count], refs[count : 2 * count], refs[2 * count]
    copies = [pltpu.make_async_copy(s, d, sem.at[k]) for k, (s, d) in enumerate(zip(srcs, dsts))]
    for copy in copies:
        copy.start()
    for copy in copies:
        copy.wait()


def copy_out(arrays):
    n = len(arrays)
    return pl.pallas_call(
        functools.partial(out_kernel, n),
        out_shape=tuple(jax.ShapeDtypeStruct(a.shape, a.dtype) for a in arrays),
        in_specs=[pl.BlockSpec(memory_space=pltpu.VMEM)] * n,
        out_specs=tuple([pl.BlockSpec(memory_space=pltpu.MemorySpace.HBM)] * n),
        scratch_shapes=[pltpu.SemaphoreType.DMA((n,))],
        compiler_params=pltpu.CompilerParams(vmem_limit_bytes=1024 * 1024),
    )(*arrays)


def shards(
    cotangent,
    layer_input,
    x_pre,
    z_pre,
    b_pre,
    c_pre,
    dt_raw,
    conv_x,
    conv_b,
    conv_c,
    dt_bias,
    a_log,
    d_skip,
    norm_w,
):
    n_sp = lax.axis_size("sp")
    n_dp = lax.axis_size("dp")
    assert x_pre.shape[0] == 1
    assert cotangent.shape[1] == BLOCK
    heads_here = dt_raw.shape[2]
    heads = heads_here * n_sp
    head_dim = x_pre.shape[2] // heads_here
    group_span = n_sp // GROUPS
    reduce_here = heads % 16 == 0 and (layer_input.shape[2] // n_dp) % LANES == 0
    args = (
        cotangent[0],
        layer_input[0],
        x_pre[0],
        z_pre[0],
        b_pre[0],
        c_pre[0],
        dt_raw[0].T,
        conv_x,
        conv_b,
        conv_c,
        dt_bias[None],
        a_log[None],
        d_skip[None],
        norm_w[None],
    )
    args = tuple(pltpu.with_memory_space_constraint(a, pltpu.MemorySpace.HBM) for a in args)
    ox, oz, ob, oc, od, oga, ow = copy_out(
        fused(args, n_sp, n_dp, group_span, head_dim, heads_here, reduce_here)
    )
    grad_a_log = oga[0]
    if not reduce_here:
        ow, grad_a_log = lax.psum((ow, grad_a_log), "dp")
        ow = lax.psum(ow, "sp")
    return ox[None], oz[None], ob[None], oc[None], od.T[None], grad_a_log, ow.T


def solution(mesh):
    placed = (
        P("dp", "sp", None),
        P("dp", "sp", None),
        P("dp", None, "sp"),
        P("dp", None, "sp"),
        P("dp", None, None),
        P("dp", None, None),
        P("dp", None, "sp"),
        P(None, "sp"),
        P(),
        P(),
        P("sp"),
        P("sp"),
        P("sp"),
        P("sp"),
    )
    return jax.shard_map(
        shards,
        mesh=mesh,
        in_specs=placed,
        out_specs=(
            P("dp", "sp", None),
            P("dp", "sp", None),
            P("dp", "sp", None),
            P("dp", "sp", None),
            P("dp", "sp", None),
            P("sp"),
            P(),
        ),
        check_vma=False,
    )
```

```python
import functools

import jax
import jax.numpy as jnp
from jax import lax
from jax.experimental import pallas as pl
from jax.experimental.pallas import tpu as pltpu
from jax.sharding import PartitionSpec as P

GROUPS = 2
STATE = 128
BLOCK = 128
LANES = 128
ROWS = 8
PAD = 8
CUT = 1
WAVE = 4
EPS = 1e-05
LOG2E = 1.4426950408889634
MESH = pl.DeviceIdType.MESH
F32 = jnp.float32
BF16 = jnp.bfloat16
ROWS_ROWS = ((1,), (1,))
COLS_COLS = ((0,), (0,))


def dot(a, b, dims=((1,), (0,)), precision=None):
    return lax.dot_general(a, b, (dims, ((), ())), precision=precision, preferred_element_type=F32)


def iota(axis, shape=(BLOCK, LANES)):
    return lax.broadcasted_iota(jnp.int32, shape, axis)


def silu_parts(u):
    sig = jax.nn.sigmoid(u)
    act = u * sig
    return act, sig + act * (1.0 - sig)


def halves(v):
    hi = v.astype(BF16)
    return jnp.concatenate([hi, (v - hi.astype(F32)).astype(BF16)], axis=1)


def add_all(parts):
    return functools.reduce(lambda a, b: a + b, parts)


def step_kernel(
    n_sp,
    n_dp,
    group_span,
    head_dim,
    heads,
    reduce_here,
    cot_hbm,
    li_hbm,
    x_hbm,
    z_hbm,
    b_hbm,
    c_hbm,
    dt_hbm,
    tapx_hbm,
    tapb_hbm,
    tapc_hbm,
    bias_hbm,
    alog_hbm,
    skip_hbm,
    nw_hbm,
    ox_ref,
    oz_ref,
    ob_ref,
    oc_ref,
    od_ref,
    oga_ref,
    ow_ref,
    cot_v,
    li_v,
    x_v,
    z_v,
    b_v,
    c_v,
    dt_v,
    tapx_v,
    tapb_v,
    tapc_v,
    bias_v,
    alog_v,
    skip_v,
    nw_v,
    cotr_s,
    xf_s,
    bf_s,
    cf_s,
    xa_s,
    gx_s,
    y_s,
    dtp_s,
    ea_s,
    te_s,
    sin_s,
    ds_s,
    st_s,
    lam_s,
    m_s,
    xdb_s,
    xdte_s,
    dy_s,
    edy_s,
    du_s,
    bb_s,
    cb_s,
    gb_s,
    gc_s,
    ct_s,
    dbu_s,
    dcu_s,
    cp_s,
    dtt_s,
    step_s,
    cum_s,
    sig_s,
    ga_s,
    acc_s,
    dyf_s,
    dsf_s,
    edyl_s,
    dz_s,
    dx_s,
    dbc_s,
    dd_s,
    rbc,
    rd,
    rga,
    part,
    rs1,
    mine1,
    rs2,
    mine2,
    rs3,
    in_sem,
    cot_send,
    cot_recv,
    z_send,
    z_recv,
    x_send,
    x_recv,
    bc_send,
    bc_recv,
    d_send,
    d_recv,
    ga_send,
    ga_recv,
    w1_send,
    w1_recv,
    w2_send,
    w2_recv,
    w3_send,
    w3_recv,
):
    pairs, length, _ = x_v.shape
    channels = pairs * LANES
    tokens = oz_ref.shape[0]
    chunks = length // BLOCK
    per = LANES // head_dim
    sp = lax.axis_index("sp")
    dp = lax.axis_index("dp")
    sp_peers = [lax.rem(sp + o, n_sp) for o in range(1, n_sp)]
    dp_peers = [lax.rem(dp + o, n_dp) for o in range(1, n_dp)] if reduce_here else []
    gcol = pl.multiple_of((sp // group_span) * STATE, STATE)
    gcols = pl.ds(gcol, STATE)

    def block(c, size=BLOCK):
        return pl.ds(pl.multiple_of(c * size, size), size)

    ours = block(sp, tokens)

    loads = {}

    def load(name, src, dst):
        loads[name] = loads.get(name, []) + [pltpu.make_async_copy(src, dst, in_sem.at[sum(map(len, loads.values()))])]
        loads[name][-1].start()

    def arrived(*names):
        for name in names:
            for copy in loads[name]:
                copy.wait()

    load("dt", dt_hbm, dt_v)
    load("dt", bias_hbm, bias_v)
    load("dt", alog_hbm, alog_v)
    load("bc", b_hbm.at[:, gcols], b_v)
    load("bc", c_hbm.at[:, gcols], c_v)
    load("bc", tapb_hbm, tapb_v)
    load("bc", tapc_hbm, tapc_v)
    load("x", tapx_hbm, tapx_v)
    load("x", skip_hbm, skip_v)
    load("x", nw_hbm, nw_v)
    for j in range(pairs):
        load("x", x_hbm.at[:, pl.ds(j * LANES, LANES)], x_v.at[j])
    load("cot", cot_hbm, cot_v)
    for j in range(pairs):
        load("z", z_hbm.at[:, pl.ds(j * LANES, LANES)], z_v.at[j])
    load("li", li_hbm, li_v)

    barrier = pltpu.get_barrier_semaphore()
    for peer in sp_peers:
        pl.semaphore_signal(barrier, inc=1, device_id={"sp": peer}, device_id_type=MESH)
    for peer in dp_peers:
        pl.semaphore_signal(barrier, inc=1, device_id={"dp": peer}, device_id_type=MESH)

    def remote(src, dst, send, recv, axis, peer):
        return pltpu.make_async_remote_copy(
            src_ref=src, dst_ref=dst, send_sem=send, recv_sem=recv,
            device_id={axis: peer}, device_id_type=MESH,
        )

    def cot_copy(peer, recv, j):
        return remote(
            cot_v.at[:, block(peer * pairs + j, LANES)], cotr_s.at[j, block(recv, tokens)],
            cot_send.at[peer, j], cot_recv.at[recv, j], "sp", peer,
        )

    def z_copy(peer, recv, j):
        return remote(
            dz_s.at[j, block(peer, tokens)], oz_ref.at[:, block(recv * pairs + j, LANES)],
            z_send.at[peer, j], z_recv.at[recv, j], "sp", peer,
        )

    def x_copy(peer, recv, j):
        return remote(
            dx_s.at[j, block(peer, tokens)], ox_ref.at[:, block(recv * pairs + j, LANES)],
            x_send.at[peer, j], x_recv.at[recv, j], "sp", peer,
        )

    def bc_copy(peer, recv):
        return remote(
            dbc_s.at[block(peer, tokens)], rbc.at[recv], bc_send.at[peer], bc_recv.at[recv], "sp", peer,
        )

    def d_copy(peer, recv):
        return remote(dd_s.at[peer], rd.at[recv], d_send.at[peer], d_recv.at[recv], "sp", peer)

    lane = iota(1)
    row = iota(0)
    half = [lane // head_dim == k for k in range(per)]
    half_b = [jnp.where(iota(1, (1, LANES)) // head_dim == k, 1.0, 0.0).astype(BF16) for k in range(per)]
    causal = row >= lane
    tri = jnp.where(causal, 1.0, 0.0).astype(BF16)
    same = jnp.where(row // head_dim == lane // head_dim, 1.0 / head_dim, 0.0).astype(BF16)
    same = jnp.concatenate([same, same], axis=0)

    def pick(parts):
        out = parts[-1]
        for k in range(per - 1):
            out = jnp.where(half[k][: out.shape[0]], parts[k], out)
        return out

    def column(v):
        v = v[...]
        n = v.shape[1]
        diag = iota(0, (ROWS, n)) == iota(1, (ROWS, n))
        return jnp.sum(jnp.where(diag, jnp.broadcast_to(v, (ROWS, n)), 0.0), axis=1, keepdims=True)

    arrived("dt")
    decay = jnp.exp(column(alog_v))
    raw = dt_v[...].astype(F32)
    if heads < ROWS:
        raw = jnp.concatenate([raw, jnp.zeros((ROWS - heads, length), F32)], axis=0)
    pre = raw + column(bias_v)
    live = iota(0, (ROWS, length)) < heads
    dt = jnp.where(live, jnp.maximum(pre, 0.0) + jnp.log1p(jnp.exp(-jnp.abs(pre))), 0.0)
    dtt_s[...] = dt
    step_s[...] = -dt * decay
    sig_s[...] = jax.nn.sigmoid(pre)
    log_step = dt * (-LOG2E * decay)
    log_step = jnp.concatenate([log_step[:, c * BLOCK : (c + 1) * BLOCK] for c in range(chunks)], axis=0)
    first = log_step.astype(BF16)
    rest = log_step - first.astype(F32)
    triu = jnp.where(row <= lane, 1.0, 0.0).astype(BF16)
    cum_s[...] = dot(
        jnp.concatenate([first, halves(rest)], axis=1), jnp.concatenate([triu, triu, triu], axis=0)
    )
    arrived("bc", "x")

    cp_s[0:1, :] = nw_v[...]
    skip = skip_v[...]
    for j in range(pairs):
        cp_s[1:2, j * LANES : (j + 1) * LANES] = pick(
            [jnp.broadcast_to(skip[0:1, j * per + k : j * per + k + 1], (1, LANES)) for k in range(per)]
        )

    zeros8 = jnp.zeros((PAD, LANES), F32)
    bf_s[0:PAD, :] = zeros8
    cf_s[0:PAD, :] = zeros8
    dbu_s[length : length + PAD, :] = zeros8
    dcu_s[length : length + PAD, :] = zeros8
    for j in range(pairs):
        xf_s[j, 0:PAD, :] = zeros8
        du_s[j, length : length + PAD, :] = zeros8
    st_s[...] = jnp.zeros_like(st_s)

    def conv(ref, base, taps):
        n = taps.shape[0]
        return add_all(
            [ref[pl.ds(base + (PAD - (n - 1 - k)), BLOCK), :] * taps[k : k + 1] for k in range(n)]
        )

    def conv_back(ref, base, taps):
        n = taps.shape[0]
        return add_all([ref[pl.ds(base + (n - 1 - k), BLOCK), :] * taps[k : k + 1] for k in range(n)])

    def forward(c, carry):
        @pl.when(c == min(CUT, chunks - 1))
        def _():
            pl.semaphore_wait(barrier, len(sp_peers) + len(dp_peers))
            arrived("cot")
            for j in range(pairs):
                for peer in sp_peers:
                    cot_copy(peer, sp, j).start()

        base = pl.multiple_of(c * BLOCK, BLOCK)
        rows = pl.ds(base, BLOCK)
        padded = pl.ds(base + PAD, BLOCK)
        bf_s[padded, :] = b_v[rows, :].astype(F32)
        cf_s[padded, :] = c_v[rows, :].astype(F32)
        for j in range(pairs):
            xf_s[j, padded, :] = x_v[j, rows, :].astype(F32)
        ba, gb = silu_parts(conv(bf_s, base, tapb_v[:, gcols].astype(F32)))
        ca, gc = silu_parts(conv(cf_s, base, tapc_v[:, gcols].astype(F32)))
        gb_s[rows, :] = gb
        gc_s[rows, :] = gc
        bb = ba.astype(BF16)
        cb = ca.astype(BF16)
        bb_s[rows, :] = bb
        cb_s[rows, :] = cb
        ct_s[rows, :] = ca.T.astype(BF16)
        b2 = halves(ba)
        c2 = halves(ca)
        c3 = jnp.concatenate([c2, cb], axis=1)
        scores = dot(c3, jnp.concatenate([bb, bb, b2[:, STATE:]], axis=1), ROWS_ROWS)
        bt2 = halves(ba.T)
        dt_c = dtt_s[:, rows]
        cum = cum_s[pl.ds(pl.multiple_of(c * ROWS, ROWS), ROWS), :]
        cols_t = jnp.concatenate([cum, dt_c, jnp.zeros((LANES - 2 * ROWS, LANES), F32)], axis=0).T
        for j in range(pairs):
            cols = pl.ds(j * LANES, LANES)
            xa, gx = silu_parts(conv(xf_s.at[j], base, tapx_v[:, cols].astype(F32)))
            gx_s[j, rows, :] = gx
            xa_s[j, rows, :] = xa
            acols, dcols, his, los = [], [], [], []
            for k in range(per):
                h = j * per + k
                acol = jnp.broadcast_to(cols_t[:, h : h + 1], (BLOCK, LANES))
                acols.append(acol)
                dcols.append(jnp.broadcast_to(cols_t[:, ROWS + h : ROWS + h + 1], (BLOCK, LANES)))
                lam = jnp.exp2(jnp.where(causal, acol - cum[h : h + 1, :], -jnp.inf))
                m = scores * lam
                hi = m.astype(BF16)
                his.append(hi)
                los.append((m - hi.astype(F32)).astype(BF16))
                lam_s[j, rows, k * BLOCK : (k + 1) * BLOCK] = lam
                m_s[j, rows, k * BLOCK : (k + 1) * BLOCK] = m
            ap = pick(acols)
            dtp = pick(dcols)
            dtp_s[j, rows, :] = dtp
            ea = jnp.exp2(ap)
            te = jnp.exp2(ap[BLOCK - 1 : BLOCK, :] - ap)
            ea_s[j, rows, :] = ea
            te_s[j, rows, :] = te
            xd = xa * dtp
            xd_hi = xd.astype(BF16)
            xd_lo = (xd - xd_hi.astype(F32)).astype(BF16)
            xdte = (xd * te).astype(BF16)
            xdb_s[j, rows, :] = xd_hi
            xdte_s[j, rows, :] = xdte
            cat_hi = [xd_hi * h for h in half_b]
            y = dot(
                jnp.concatenate(his + los + his, axis=1),
                jnp.concatenate(cat_hi + cat_hi + [xd_lo * h for h in half_b], axis=0),
            )
            st = st_s[j]
            sin_s[j, rows, :] = st
            st_hi = st.astype(BF16)
            st_lo = (st - st_hi.astype(F32)).astype(BF16)
            y_s[j, rows, :] = y + dot(c3, jnp.concatenate([st_hi, st_hi, st_lo], axis=0)) * ea
            st_s[j] = st * ea[BLOCK - 1 : BLOCK, :] + dot(bt2, jnp.concatenate([xdte, xdte], axis=0))
        return carry

    lax.fori_loop(0, chunks, forward, 0)

    for j in range(pairs):
        cotr_s[j, ours, :] = cot_v[:, block(sp * pairs + j, LANES)]
    arrived("z")
    acc_s[...] = jnp.zeros_like(acc_s)

    def middle(j, carry):
        cols = block(j, LANES)
        for peer in sp_peers:
            cot_copy(peer, peer, j).wait_recv()

        @pl.when(j > 0)
        def _():
            for peer in sp_peers:
                z_copy(peer, sp, j - 1).start()

        gain = cp_s[0:1, cols]
        skips = cp_s[1:2, cols]
        place_r = jnp.where(row // head_dim + j * per == lane, 1.0, 0.0).astype(BF16)
        place_q = jnp.where(row // head_dim + (j * per + LANES // 2) == lane, 1.0, 0.0).astype(BF16)
        place_r = jnp.concatenate([place_r, place_r], axis=0)
        for start in range(0, chunks, WAVE):
            wave = list(reversed(range(chunks)))[start : start + WAVE]
            state = []
            for c in wave:
                rows = pl.ds(c * BLOCK, BLOCK)
                full = y_s[j, rows, :] + skips * xa_s[j, rows, :]
                sz, gz = silu_parts(z_v[j, rows, :].astype(F32))
                gated = full * sz
                state.append((full, sz, gz, gated, dot(halves(gated * gated), same)))
            means = []
            for c, (full, sz, gz, gated, power) in zip(wave, state):
                inv = lax.rsqrt(power + EPS)
                gh = gated * inv
                g = cotr_s[j, pl.ds(c * BLOCK, BLOCK), :].astype(F32) * gain
                means.append((inv, gh, g, dot(halves(g * gh), same)))
            for c, (full, sz, gz, gated, _), (inv, gh, g, mean) in zip(wave, state, means):
                rows = pl.ds(c * BLOCK, BLOCK)
                dgated = inv * (g - gh * mean)
                dz_s[j, rows, :] = (dgated * full * gz).astype(BF16)
                dy = dgated * sz
                dyf_s[rows, :] = dy
                dy_s[j, rows, :] = halves(dy)
                edy = ea_s[j, rows, :] * dy
                edy_hi = edy.astype(BF16)
                edy_s[j, rows, :] = edy_hi
                edyl_s[rows, :] = (edy - edy_hi.astype(F32)).astype(BF16)
        ds = jnp.zeros((STATE, LANES), F32)
        for c in reversed(range(chunks)):
            rows = pl.ds(c * BLOCK, BLOCK)
            dsf_s[rows, :] = ds
            ds_hi = ds.astype(BF16)
            ds_s[j, rows, :] = ds_hi
            if c > 0:
                last = pl.ds(c * BLOCK + BLOCK - 1, 1)
                ct = ct_s[rows, :]
                ds = ds * ea_s[j, last, :] + dot(
                    jnp.concatenate([ct, ct], axis=1),
                    jnp.concatenate([edy_s[j, rows, :], edyl_s[rows, :]], axis=0),
                )
        for c in reversed(range(chunks)):
            rows = pl.ds(c * BLOCK, BLOCK)
            dy2 = dy_s[j, rows, :]
            mt2 = halves(
                jnp.concatenate([m_s[j, rows, k * BLOCK : (k + 1) * BLOCK].T for k in range(per)], axis=1)
            )
            dycat = [dy2[:, p * LANES : (p + 1) * LANES] * h for p in range(2) for h in half_b]
            bb = bb_s[rows, :]
            dstate = te_s[j, rows, :] * dot(
                bb, ds_s[j, rows, :]
            )
            mt3 = jnp.concatenate([mt2[:, : per * BLOCK], mt2], axis=1)
            dxd = dot(mt3, jnp.concatenate(dycat[per:] + dycat[:per] + dycat[:per], axis=0)) + dstate
            xa = xa_s[j, rows, :]
            dtp = dtp_s[j, rows, :]
            dy = dyf_s[rows, :]
            tail = jnp.sum(xa * dtp * dstate, axis=0, keepdims=True) + ea_s[
                j, pl.ds(c * BLOCK + BLOCK - 1, 1), :
            ] * jnp.sum(dsf_s[rows, :] * sin_s[j, rows, :], axis=0, keepdims=True)
            q = dxd * xa
            r = dy * y_s[j, rows, :] - q * dtp
            r = jnp.concatenate(
                [
                    r[: BLOCK - ROWS],
                    r[BLOCK - ROWS :] + jnp.where(iota(0, (ROWS, LANES)) == ROWS - 1, tail, 0.0),
                ],
                axis=0,
            )
            acc_s[rows, :] = acc_s[rows, :] + dot(halves(r), place_r) + dot(q.astype(BF16), place_q)
            du_s[j, rows, :] = (dxd * dtp + skips * dy) * gx_s[j, rows, :]
        return carry

    lax.fori_loop(0, pairs, middle, 0)

    acc_t = [acc_s[pl.ds(c * BLOCK, BLOCK), :].T for c in range(chunks)]
    dlogs = dot(
        halves(jnp.concatenate([t[0:ROWS] for t in acc_t], axis=0)), jnp.concatenate([tri, tri], axis=0)
    )
    ga = jnp.zeros((ROWS, LANES), F32)
    for c in range(chunks):
        rows = pl.ds(c * BLOCK, BLOCK)
        dlog = dlogs[c * ROWS : (c + 1) * ROWS]
        ddt = acc_t[c][LANES // 2 : LANES // 2 + ROWS] - dlog * decay
        dd_s[c] = (ddt * sig_s[:, rows]).astype(BF16)
        ga = ga + dlog * step_s[:, rows]
    for peer in sp_peers:
        d_copy(peer, sp).start()
    for peer in sp_peers:
        z_copy(peer, sp, pairs - 1).start()
    ga_col = jnp.sum(ga, axis=1, keepdims=True)

    def ga_row(col):
        diag = iota(0, (ROWS, heads)) == iota(1, (ROWS, heads))
        return jnp.sum(jnp.where(diag, jnp.broadcast_to(col, (ROWS, heads)), 0.0), axis=0, keepdims=True)

    def ga_copy(peer, recv):
        return remote(ga_s, rga.at[recv], ga_send.at[peer], ga_recv.at[recv], "dp", peer)

    if reduce_here:
        ga_s[...] = jnp.broadcast_to(ga_col, ga_s.shape)
        for peer in dp_peers:
            ga_copy(peer, dp).start()
    else:
        oga_ref[...] = ga_row(ga_col)

    def convolve(i, carry):
        c = chunks - 1 - i
        base = pl.multiple_of(c * BLOCK, BLOCK)
        rows = pl.ds(base, BLOCK)
        for j in range(pairs):
            cols = pl.ds(j * LANES, LANES)
            dx_s[j, rows, :] = conv_back(du_s.at[j], base, tapx_v[:, cols].astype(F32)).astype(BF16)
        return carry

    lax.fori_loop(0, chunks, convolve, 0)
    early = pairs // 2 if reduce_here else pairs
    for j in range(early):
        for peer in sp_peers:
            x_copy(peer, sp, j).start()

    def backward(i, carry):
        c = chunks - 1 - i
        base = pl.multiple_of(c * BLOCK, BLOCK)
        rows = pl.ds(base, BLOCK)
        dscores = jnp.zeros((BLOCK, BLOCK), F32)
        dcc = jnp.zeros((BLOCK, STATE), F32)
        dbb = jnp.zeros((BLOCK, STATE), F32)
        for j in range(pairs):
            cols = pl.ds(j * LANES, LANES)
            xdb = xdb_s[j, rows, :]
            xcat = jnp.concatenate([xdb * h for h in half_b], axis=0)
            dm = dot(dy_s[j, rows, :], jnp.concatenate([xcat, xcat], axis=1), ROWS_ROWS) * lam_s[j, rows, :]
            for k in range(per):
                dscores = dscores + dm[:, k * BLOCK : (k + 1) * BLOCK]

        def joined(ref):
            return jnp.concatenate([ref[j, rows, :].astype(BF16) for j in range(pairs)], axis=1)

        dcc = dot(joined(edy_s), joined(sin_s), ROWS_ROWS)
        dbb = dot(joined(xdte_s), joined(ds_s), ROWS_ROWS)
        dcc = dcc + dot(dscores.astype(BF16), bb_s[rows, :])
        dbb = dbb + dot(dscores.T.astype(BF16), cb_s[rows, :])
        dbu_s[rows, :] = dbb * gb_s[rows, :]
        dcu_s[rows, :] = dcc * gc_s[rows, :]
        dbc_s[rows, 0:STATE] = conv_back(dbu_s, base, tapb_v[:, gcols].astype(F32)).astype(BF16)
        dbc_s[rows, STATE : 2 * STATE] = conv_back(dcu_s, base, tapc_v[:, gcols].astype(F32)).astype(BF16)
        return carry

    mid = chunks // 2
    lax.fori_loop(0, mid, backward, 0)

    rd[sp] = dd_s[sp]
    for peer in sp_peers:
        d_copy(peer, peer).wait_recv()
    whole_d = jnp.concatenate([rd[k].astype(F32)[:heads] for k in range(n_sp)], axis=0).astype(BF16)
    od_ref[...] = whole_d
    arrived("li")
    whole_w = dot(whole_d, li_v[...])

    if reduce_here:
        width = part.shape[1] // n_dp

        def w1_copy(peer, recv):
            return remote(
                part.at[:, block(peer, width)], rs1.at[recv], w1_send.at[peer], w1_recv.at[recv], "dp", peer
            )

        def w2_copy(peer, recv):
            return remote(mine1, rs2.at[recv], w2_send.at[peer], w2_recv.at[recv], "sp", peer)

        def w3_copy(peer, recv):
            return remote(mine2, rs3.at[recv], w3_send.at[peer], w3_recv.at[recv], "dp", peer)

        part[...] = whole_w.astype(BF16)
        for peer in dp_peers:
            w1_copy(peer, dp).start()
        rs1[dp] = part[:, block(dp, width)]
    else:
        ow_ref[...] = whole_w

    lax.fori_loop(mid, chunks, backward, 0)

    if reduce_here:
        for peer in dp_peers:
            w1_copy(peer, peer).wait_recv()
        mine1[...] = add_all([rs1[k].astype(F32) for k in range(n_dp)]).astype(BF16)
        for peer in sp_peers:
            w2_copy(peer, sp).start()
        for j in range(early, pairs):
            for peer in sp_peers:
                x_copy(peer, sp, j).start()
        for peer in sp_peers:
            bc_copy(peer, sp).start()
        rs2[sp] = mine1[...]
        rga[dp] = ga_s[...]
        for peer in dp_peers:
            ga_copy(peer, peer).wait_recv()
        oga_ref[...] = ga_row(add_all([rga[k] for k in range(n_dp)])[:, 0:1])
        for peer in sp_peers:
            w2_copy(peer, peer).wait_recv()
        mine2[...] = add_all([rs2[k].astype(F32) for k in range(n_sp)]).astype(BF16)
        for peer in dp_peers:
            w3_copy(peer, dp).start()
        rs3[dp] = mine2[...]

    else:
        for peer in sp_peers:
            bc_copy(peer, sp).start()
    for j in range(pairs):
        oz_ref[:, block(sp * pairs + j, LANES)] = dz_s[j, ours, :]
        ox_ref[:, block(sp * pairs + j, LANES)] = dx_s[j, ours, :]
    rbc[sp] = dbc_s[ours, :]
    for peer in sp_peers:
        d_copy(peer, sp).wait_send()
        for j in range(pairs):
            cot_copy(peer, sp, j).wait_send()
            z_copy(peer, sp, j).wait_send()
            z_copy(peer, peer, j).wait_recv()
        for j in range(early):
            x_copy(peer, peer, j).wait_recv()
            x_copy(peer, sp, j).wait_send()
    for peer in dp_peers:
        ga_copy(peer, dp).wait_send()
        w1_copy(peer, dp).wait_send()
    for peer in sp_peers:
        if reduce_here:
            w2_copy(peer, sp).wait_send()
        for j in range(early, pairs):
            x_copy(peer, peer, j).wait_recv()
            x_copy(peer, sp, j).wait_send()
    for peer in sp_peers:
        bc_copy(peer, peer).wait_recv()
        bc_copy(peer, sp).wait_send()
    for g in range(GROUPS):
        total = add_all([rbc[g * group_span + k].astype(F32) for k in range(group_span)]).astype(BF16)
        ob_ref[:, g * STATE : (g + 1) * STATE] = total[:, 0:STATE]
        oc_ref[:, g * STATE : (g + 1) * STATE] = total[:, STATE : 2 * STATE]
    if reduce_here:
        for peer in dp_peers:
            w3_copy(peer, peer).wait_recv()
            w3_copy(peer, dp).wait_send()
        for k in range(n_dp):
            ow_ref[:, k * width : (k + 1) * width] = rs3[k].astype(F32)


def fused(args, n_sp, n_dp, group_span, head_dim, heads, reduce_here):
    cot, li, x, z, b, c, dt, tapx, tapb, tapc, bias, alog, skip, nw = args
    length, channels = x.shape
    tokens, width = li.shape
    all_heads = heads * n_sp
    per = LANES // head_dim
    pairs = channels // LANES
    vm = pltpu.VMEM
    dma = pltpu.SemaphoreType.DMA
    wide = vm((pairs, length, LANES), F32)
    wide_b = vm((pairs, length, LANES), BF16)
    thin = vm((length, LANES), F32)
    thin_b = vm((length, LANES), BF16)
    padded = vm((length + PAD, LANES), F32)
    tall = vm((pairs, length + PAD, LANES), F32)
    rows = vm((ROWS, length), F32)
    piece = width // n_dp if reduce_here else LANES
    return pl.pallas_call(
        functools.partial(step_kernel, n_sp, n_dp, group_span, head_dim, heads, reduce_here),
        out_shape=(
            jax.ShapeDtypeStruct((tokens, channels * n_sp), BF16),
            jax.ShapeDtypeStruct((tokens, channels * n_sp), BF16),
            jax.ShapeDtypeStruct((tokens, GROUPS * STATE), BF16),
            jax.ShapeDtypeStruct((tokens, GROUPS * STATE), BF16),
            jax.ShapeDtypeStruct((all_heads, tokens), BF16),
            jax.ShapeDtypeStruct((1, heads), F32),
            jax.ShapeDtypeStruct((all_heads, width), F32),
        ),
        in_specs=[pl.BlockSpec(memory_space=pltpu.MemorySpace.HBM)] * 14,
        out_specs=tuple([pl.BlockSpec(memory_space=pltpu.VMEM)] * 7),
        scratch_shapes=[
            vm((tokens, channels * n_sp), BF16),
            vm((tokens, width), BF16),
            wide_b,
            wide_b,
            thin_b,
            thin_b,
            vm((heads, length), BF16),
            vm(tapx.shape, BF16),
            vm(tapb.shape, BF16),
            vm(tapc.shape, BF16),
            vm((1, heads), F32),
            vm((1, heads), F32),
            vm((1, heads), F32),
            vm((1, channels), F32),
            wide_b,
            tall,
            padded,
            padded,
            wide,
            wide,
            wide,
            wide,
            wide,
            wide,
            wide,
            wide_b,
            vm((pairs, STATE, LANES), F32),
            vm((pairs, length, per * BLOCK), F32),
            vm((pairs, length, per * BLOCK), F32),
            wide_b,
            wide_b,
            vm((pairs, length, 2 * LANES), BF16),
            wide_b,
            tall,
            thin_b,
            thin_b,
            thin,
            thin,
            thin_b,
            padded,
            padded,
            vm((ROWS, channels), F32),
            rows,
            rows,
            vm((length // BLOCK * ROWS, LANES), F32),
            rows,
            vm((ROWS, LANES), F32),
            thin,
            thin,
            thin,
            thin_b,
            wide_b,
            wide_b,
            vm((length, 2 * STATE), BF16),
            vm((length // BLOCK, ROWS, BLOCK), BF16),
            vm((n_sp, tokens, 2 * STATE), BF16),
            vm((n_sp, ROWS, BLOCK), BF16),
            vm((n_dp, ROWS, LANES), F32),
            vm((all_heads, width), BF16),
            vm((n_dp, all_heads, piece), BF16),
            vm((all_heads, piece), BF16),
            vm((n_sp, all_heads, piece), BF16),
            vm((all_heads, piece), BF16),
            vm((n_dp, all_heads, piece), BF16),
            dma((12 + 2 * pairs,)),
        ]
        + [dma((n_sp, pairs))] * 6
        + [dma((n_sp,))] * 4
        + [dma((n_dp,))] * 4
        + [dma((n_sp,))] * 2
        + [dma((n_dp,))] * 2,
        compiler_params=pltpu.CompilerParams(
            collective_id=0, has_side_effects=True, vmem_limit_bytes=40 * 1024 * 1024
        ),
    )(*args)


def out_kernel(count, *refs):
    srcs, dsts, sem = refs[:count], refs[count : 2 * count], refs[2 * count]
    copies = [pltpu.make_async_copy(s, d, sem.at[k]) for k, (s, d) in enumerate(zip(srcs, dsts))]
    for copy in copies:
        copy.start()
    for copy in copies:
        copy.wait()


def copy_out(arrays):
    n = len(arrays)
    return pl.pallas_call(
        functools.partial(out_kernel, n),
        out_shape=tuple(jax.ShapeDtypeStruct(a.shape, a.dtype) for a in arrays),
        in_specs=[pl.BlockSpec(memory_space=pltpu.VMEM)] * n,
        out_specs=tuple([pl.BlockSpec(memory_space=pltpu.MemorySpace.HBM)] * n),
        scratch_shapes=[pltpu.SemaphoreType.DMA((n,))],
        compiler_params=pltpu.CompilerParams(vmem_limit_bytes=1024 * 1024),
    )(*arrays)


def shards(
    cotangent,
    layer_input,
    x_pre,
    z_pre,
    b_pre,
    c_pre,
    dt_raw,
    conv_x,
    conv_b,
    conv_c,
    dt_bias,
    a_log,
    d_skip,
    norm_w,
):
    n_sp = lax.axis_size("sp")
    n_dp = lax.axis_size("dp")
    assert x_pre.shape[0] == 1
    assert cotangent.shape[1] == BLOCK
    heads_here = dt_raw.shape[2]
    heads = heads_here * n_sp
    head_dim = x_pre.shape[2] // heads_here
    group_span = n_sp // GROUPS
    reduce_here = heads % 16 == 0 and (layer_input.shape[2] // n_dp) % LANES == 0
    args = (
        cotangent[0],
        layer_input[0],
        x_pre[0],
        z_pre[0],
        b_pre[0],
        c_pre[0],
        dt_raw[0].T,
        conv_x,
        conv_b,
        conv_c,
        dt_bias[None],
        a_log[None],
        d_skip[None],
        norm_w[None],
    )
    args = tuple(pltpu.with_memory_space_constraint(a, pltpu.MemorySpace.HBM) for a in args)
    ox, oz, ob, oc, od, oga, ow = copy_out(
        fused(args, n_sp, n_dp, group_span, head_dim, heads_here, reduce_here)
    )
    grad_a_log = oga[0]
    if not reduce_here:
        ow, grad_a_log = lax.psum((ow, grad_a_log), "dp")
        ow = lax.psum(ow, "sp")
    return ox[None], oz[None], ob[None], oc[None], od.T[None], grad_a_log, ow.T


def solution(mesh):
    placed = (
        P("dp", "sp", None),
        P("dp", "sp", None),
        P("dp", None, "sp"),
        P("dp", None, "sp"),
        P("dp", None, None),
        P("dp", None, None),
        P("dp", None, "sp"),
        P(None, "sp"),
        P(),
        P(),
        P("sp"),
        P("sp"),
        P("sp"),
        P("sp"),
    )
    return jax.shard_map(
        shards,
        mesh=mesh,
        in_specs=placed,
        out_specs=(
            P("dp", "sp", None),
            P("dp", "sp", None),
            P("dp", "sp", None),
            P("dp", "sp", None),
            P("dp", "sp", None),
            P("sp"),
            P(),
        ),
        check_vma=False,
    )
```

```python
import functools

import jax
import jax.numpy as jnp
from jax import lax
from jax.experimental import pallas as pl
from jax.experimental.pallas import tpu as pltpu
from jax.sharding import PartitionSpec as P

GROUPS = 2
STATE = 128
BLOCK = 128
LANES = 128
ROWS = 8
PAD = 8
CUT = 1
WAVE = 4
EPS = 1e-05
LOG2E = 1.4426950408889634
MESH = pl.DeviceIdType.MESH
F32 = jnp.float32
BF16 = jnp.bfloat16
ROWS_ROWS = ((1,), (1,))
COLS_COLS = ((0,), (0,))


def dot(a, b, dims=((1,), (0,)), precision=None):
    return lax.dot_general(a, b, (dims, ((), ())), precision=precision, preferred_element_type=F32)


def iota(axis, shape=(BLOCK, LANES)):
    return lax.broadcasted_iota(jnp.int32, shape, axis)


def silu_parts(u):
    sig = jax.nn.sigmoid(u)
    act = u * sig
    return act, sig + act * (1.0 - sig)


def halves(v):
    hi = v.astype(BF16)
    return jnp.concatenate([hi, (v - hi.astype(F32)).astype(BF16)], axis=1)


def add_all(parts):
    return functools.reduce(lambda a, b: a + b, parts)


def step_kernel(
    n_sp,
    n_dp,
    group_span,
    head_dim,
    heads,
    reduce_here,
    cot_hbm,
    li_hbm,
    x_hbm,
    z_hbm,
    b_hbm,
    c_hbm,
    dt_hbm,
    tapx_hbm,
    tapb_hbm,
    tapc_hbm,
    bias_hbm,
    alog_hbm,
    skip_hbm,
    nw_hbm,
    ox_ref,
    oz_ref,
    ob_ref,
    oc_ref,
    od_ref,
    oga_ref,
    ow_ref,
    cot_v,
    li_v,
    x_v,
    z_v,
    b_v,
    c_v,
    dt_v,
    tapx_v,
    tapb_v,
    tapc_v,
    bias_v,
    alog_v,
    skip_v,
    nw_v,
    cotr_s,
    xf_s,
    bf_s,
    cf_s,
    xa_s,
    gx_s,
    y_s,
    dtp_s,
    ea_s,
    te_s,
    sin_s,
    ds_s,
    st_s,
    lam_s,
    m_s,
    xdb_s,
    xdte_s,
    dy_s,
    edy_s,
    du_s,
    bb_s,
    cb_s,
    gb_s,
    gc_s,
    ct_s,
    dbu_s,
    dcu_s,
    cp_s,
    dtt_s,
    step_s,
    cum_s,
    sig_s,
    ga_s,
    acc_s,
    dyf_s,
    dsf_s,
    edyl_s,
    dz_s,
    dx_s,
    dbc_s,
    dd_s,
    rbc,
    rd,
    rga,
    part,
    rs1,
    mine1,
    rs2,
    mine2,
    rs3,
    in_sem,
    cot_send,
    cot_recv,
    z_send,
    z_recv,
    x_send,
    x_recv,
    bc_send,
    bc_recv,
    d_send,
    d_recv,
    ga_send,
    ga_recv,
    w1_send,
    w1_recv,
    w2_send,
    w2_recv,
    w3_send,
    w3_recv,
):
    pairs, length, _ = x_v.shape
    channels = pairs * LANES
    tokens = oz_ref.shape[0]
    chunks = length // BLOCK
    per = LANES // head_dim
    sp = lax.axis_index("sp")
    dp = lax.axis_index("dp")
    sp_peers = [lax.rem(sp + o, n_sp) for o in range(1, n_sp)]
    dp_peers = [lax.rem(dp + o, n_dp) for o in range(1, n_dp)] if reduce_here else []
    gcol = pl.multiple_of((sp // group_span) * STATE, STATE)
    gcols = pl.ds(gcol, STATE)

    def block(c, size=BLOCK):
        return pl.ds(pl.multiple_of(c * size, size), size)

    ours = block(sp, tokens)

    loads = {}

    def load(name, src, dst):
        loads[name] = loads.get(name, []) + [pltpu.make_async_copy(src, dst, in_sem.at[sum(map(len, loads.values()))])]
        loads[name][-1].start()

    def arrived(*names):
        for name in names:
            for copy in loads[name]:
                copy.wait()

    load("dt", dt_hbm, dt_v)
    load("dt", bias_hbm, bias_v)
    load("dt", alog_hbm, alog_v)
    load("bc", b_hbm.at[:, gcols], b_v)
    load("bc", c_hbm.at[:, gcols], c_v)
    load("bc", tapb_hbm, tapb_v)
    load("bc", tapc_hbm, tapc_v)
    load("x", tapx_hbm, tapx_v)
    load("x", skip_hbm, skip_v)
    load("x", nw_hbm, nw_v)
    for j in range(pairs):
        load("x", x_hbm.at[:, pl.ds(j * LANES, LANES)], x_v.at[j])
    load("cot", cot_hbm, cot_v)
    for j in range(pairs):
        load("z", z_hbm.at[:, pl.ds(j * LANES, LANES)], z_v.at[j])
    load("li", li_hbm, li_v)

    barrier = pltpu.get_barrier_semaphore()
    for peer in sp_peers:
        pl.semaphore_signal(barrier, inc=1, device_id={"sp": peer}, device_id_type=MESH)
    for peer in dp_peers:
        pl.semaphore_signal(barrier, inc=1, device_id={"dp": peer}, device_id_type=MESH)

    def remote(src, dst, send, recv, axis, peer):
        return pltpu.make_async_remote_copy(
            src_ref=src, dst_ref=dst, send_sem=send, recv_sem=recv,
            device_id={axis: peer}, device_id_type=MESH,
        )

    def cot_copy(peer, recv, j):
        return remote(
            cot_v.at[:, block(peer * pairs + j, LANES)], cotr_s.at[j, block(recv, tokens)],
            cot_send.at[peer, j], cot_recv.at[recv, j], "sp", peer,
        )

    def z_copy(peer, recv, j):
        return remote(
            dz_s.at[j, block(peer, tokens)], oz_ref.at[:, block(recv * pairs + j, LANES)],
            z_send.at[peer, j], z_recv.at[recv, j], "sp", peer,
        )

    def x_copy(peer, recv, j):
        return remote(
            dx_s.at[j, block(peer, tokens)], ox_ref.at[:, block(recv * pairs + j, LANES)],
            x_send.at[peer, j], x_recv.at[recv, j], "sp", peer,
        )

    def bc_copy(peer, recv):
        return remote(
            dbc_s.at[block(peer, tokens)], rbc.at[recv], bc_send.at[peer], bc_recv.at[recv], "sp", peer,
        )

    def d_copy(peer, recv):
        return remote(dd_s.at[peer], rd.at[recv], d_send.at[peer], d_recv.at[recv], "sp", peer)

    lane = iota(1)
    row = iota(0)
    half = [lane // head_dim == k for k in range(per)]
    half_b = [jnp.where(iota(1, (1, LANES)) // head_dim == k, 1.0, 0.0).astype(BF16) for k in range(per)]
    causal = row >= lane
    tri = jnp.where(causal, 1.0, 0.0).astype(BF16)
    same = jnp.where(row // head_dim == lane // head_dim, 1.0 / head_dim, 0.0).astype(BF16)
    same = jnp.concatenate([same, same], axis=0)

    def pick(parts):
        out = parts[-1]
        for k in range(per - 1):
            out = jnp.where(half[k][: out.shape[0]], parts[k], out)
        return out

    def column(v):
        v = v[...]
        n = v.shape[1]
        diag = iota(0, (ROWS, n)) == iota(1, (ROWS, n))
        return jnp.sum(jnp.where(diag, jnp.broadcast_to(v, (ROWS, n)), 0.0), axis=1, keepdims=True)

    arrived("dt")
    decay = jnp.exp(column(alog_v))
    raw = dt_v[...].astype(F32)
    if heads < ROWS:
        raw = jnp.concatenate([raw, jnp.zeros((ROWS - heads, length), F32)], axis=0)
    pre = raw + column(bias_v)
    live = iota(0, (ROWS, length)) < heads
    dt = jnp.where(live, jnp.maximum(pre, 0.0) + jnp.log1p(jnp.exp(-jnp.abs(pre))), 0.0)
    dtt_s[...] = dt
    step_s[...] = -dt * decay
    sig_s[...] = jax.nn.sigmoid(pre)
    log_step = dt * (-LOG2E * decay)
    log_step = jnp.concatenate([log_step[:, c * BLOCK : (c + 1) * BLOCK] for c in range(chunks)], axis=0)
    first = log_step.astype(BF16)
    rest = log_step - first.astype(F32)
    triu = jnp.where(row <= lane, 1.0, 0.0).astype(BF16)
    cum_s[...] = dot(
        jnp.concatenate([first, halves(rest)], axis=1), jnp.concatenate([triu, triu, triu], axis=0)
    )
    arrived("bc", "x")

    cp_s[0:1, :] = nw_v[...]
    skip = skip_v[...]
    for j in range(pairs):
        cp_s[1:2, j * LANES : (j + 1) * LANES] = pick(
            [jnp.broadcast_to(skip[0:1, j * per + k : j * per + k + 1], (1, LANES)) for k in range(per)]
        )

    zeros8 = jnp.zeros((PAD, LANES), F32)
    bf_s[0:PAD, :] = zeros8
    cf_s[0:PAD, :] = zeros8
    dbu_s[length : length + PAD, :] = zeros8
    dcu_s[length : length + PAD, :] = zeros8
    for j in range(pairs):
        xf_s[j, 0:PAD, :] = zeros8
        du_s[j, length : length + PAD, :] = zeros8
    st_s[...] = jnp.zeros_like(st_s)

    def conv(ref, base, taps):
        n = taps.shape[0]
        return add_all(
            [ref[pl.ds(base + (PAD - (n - 1 - k)), BLOCK), :] * taps[k : k + 1] for k in range(n)]
        )

    def conv_back(ref, base, taps):
        n = taps.shape[0]
        return add_all([ref[pl.ds(base + (n - 1 - k), BLOCK), :] * taps[k : k + 1] for k in range(n)])

    def forward(c, carry):
        @pl.when(c == min(CUT, chunks - 1))
        def _():
            pl.semaphore_wait(barrier, len(sp_peers) + len(dp_peers))
            arrived("cot")
            for j in range(pairs):
                for peer in sp_peers:
                    cot_copy(peer, sp, j).start()

        base = pl.multiple_of(c * BLOCK, BLOCK)
        rows = pl.ds(base, BLOCK)
        padded = pl.ds(base + PAD, BLOCK)
        bf_s[padded, :] = b_v[rows, :].astype(F32)
        cf_s[padded, :] = c_v[rows, :].astype(F32)
        for j in range(pairs):
            xf_s[j, padded, :] = x_v[j, rows, :].astype(F32)
        ba, gb = silu_parts(conv(bf_s, base, tapb_v[:, gcols].astype(F32)))
        ca, gc = silu_parts(conv(cf_s, base, tapc_v[:, gcols].astype(F32)))
        gb_s[rows, :] = gb
        gc_s[rows, :] = gc
        bb = ba.astype(BF16)
        cb = ca.astype(BF16)
        bb_s[rows, :] = bb
        cb_s[rows, :] = cb
        ct_s[rows, :] = ca.T.astype(BF16)
        b2 = halves(ba)
        c2 = halves(ca)
        c3 = jnp.concatenate([c2, cb], axis=1)
        scores = dot(c3, jnp.concatenate([bb, bb, b2[:, STATE:]], axis=1), ROWS_ROWS)
        bt2 = halves(ba.T)
        dt_c = dtt_s[:, rows]
        cum = cum_s[pl.ds(pl.multiple_of(c * ROWS, ROWS), ROWS), :]
        cols_t = jnp.concatenate([cum, dt_c, jnp.zeros((LANES - 2 * ROWS, LANES), F32)], axis=0).T
        for j in range(pairs):
            cols = pl.ds(j * LANES, LANES)
            xa, gx = silu_parts(conv(xf_s.at[j], base, tapx_v[:, cols].astype(F32)))
            gx_s[j, rows, :] = gx
            xa_s[j, rows, :] = xa
            acols, dcols, his, los = [], [], [], []
            for k in range(per):
                h = j * per + k
                acol = jnp.broadcast_to(cols_t[:, h : h + 1], (BLOCK, LANES))
                acols.append(acol)
                dcols.append(jnp.broadcast_to(cols_t[:, ROWS + h : ROWS + h + 1], (BLOCK, LANES)))
                lam = jnp.exp2(jnp.where(causal, acol - cum[h : h + 1, :], -jnp.inf))
                m = scores * lam
                hi = m.astype(BF16)
                his.append(hi)
                los.append((m - hi.astype(F32)).astype(BF16))
                lam_s[j, rows, k * BLOCK : (k + 1) * BLOCK] = lam
                m_s[j, rows, k * BLOCK : (k + 1) * BLOCK] = m
            ap = pick(acols)
            dtp = pick(dcols)
            dtp_s[j, rows, :] = dtp
            ea = jnp.exp2(ap)
            te = jnp.exp2(ap[BLOCK - 1 : BLOCK, :] - ap)
            ea_s[j, rows, :] = ea
            te_s[j, rows, :] = te
            xd = xa * dtp
            xd_hi = xd.astype(BF16)
            xd_lo = (xd - xd_hi.astype(F32)).astype(BF16)
            xdte = (xd * te).astype(BF16)
            xdb_s[j, rows, :] = xd_hi
            xdte_s[j, rows, :] = xdte
            cat_hi = [xd_hi * h for h in half_b]
            y = dot(
                jnp.concatenate(his + los + his, axis=1),
                jnp.concatenate(cat_hi + cat_hi + [xd_lo * h for h in half_b], axis=0),
            )
            st = st_s[j]
            sin_s[j, rows, :] = st
            st_hi = st.astype(BF16)
            st_lo = (st - st_hi.astype(F32)).astype(BF16)
            y_s[j, rows, :] = y + dot(c3, jnp.concatenate([st_hi, st_hi, st_lo], axis=0)) * ea
            st_s[j] = st * ea[BLOCK - 1 : BLOCK, :] + dot(bt2, jnp.concatenate([xdte, xdte], axis=0))
        return carry

    lax.fori_loop(0, chunks, forward, 0)

    for j in range(pairs):
        cotr_s[j, ours, :] = cot_v[:, block(sp * pairs + j, LANES)]
    arrived("z")
    acc_s[...] = jnp.zeros_like(acc_s)

    def middle(j, carry):
        cols = block(j, LANES)
        for peer in sp_peers:
            cot_copy(peer, peer, j).wait_recv()

        @pl.when(j > 0)
        def _():
            for peer in sp_peers:
                z_copy(peer, sp, j - 1).start()

        gain = cp_s[0:1, cols]
        skips = cp_s[1:2, cols]
        place_r = jnp.where(row // head_dim + j * per == lane, 1.0, 0.0).astype(BF16)
        place_q = jnp.where(row // head_dim + (j * per + LANES // 2) == lane, 1.0, 0.0).astype(BF16)
        place_r = jnp.concatenate([place_r, place_r], axis=0)
        for start in range(0, chunks, WAVE):
            wave = list(reversed(range(chunks)))[start : start + WAVE]
            state = []
            for c in wave:
                rows = pl.ds(c * BLOCK, BLOCK)
                full = y_s[j, rows, :] + skips * xa_s[j, rows, :]
                sz, gz = silu_parts(z_v[j, rows, :].astype(F32))
                gated = full * sz
                state.append((full, sz, gz, gated, dot(halves(gated * gated), same)))
            means = []
            for c, (full, sz, gz, gated, power) in zip(wave, state):
                inv = lax.rsqrt(power + EPS)
                gh = gated * inv
                g = cotr_s[j, pl.ds(c * BLOCK, BLOCK), :].astype(F32) * gain
                means.append((inv, gh, g, dot(halves(g * gh), same)))
            for c, (full, sz, gz, gated, _), (inv, gh, g, mean) in zip(wave, state, means):
                rows = pl.ds(c * BLOCK, BLOCK)
                dgated = inv * (g - gh * mean)
                dz_s[j, rows, :] = (dgated * full * gz).astype(BF16)
                dy = dgated * sz
                dyf_s[rows, :] = dy
                dy_s[j, rows, :] = halves(dy)
                edy = ea_s[j, rows, :] * dy
                edy_hi = edy.astype(BF16)
                edy_s[j, rows, :] = edy_hi
                edyl_s[rows, :] = (edy - edy_hi.astype(F32)).astype(BF16)
        ds = jnp.zeros((STATE, LANES), F32)
        for c in reversed(range(chunks)):
            rows = pl.ds(c * BLOCK, BLOCK)
            dsf_s[rows, :] = ds
            ds_hi = ds.astype(BF16)
            ds_s[j, rows, :] = ds_hi
            if c > 0:
                last = pl.ds(c * BLOCK + BLOCK - 1, 1)
                ct = ct_s[rows, :]
                ds = ds * ea_s[j, last, :] + dot(
                    jnp.concatenate([ct, ct], axis=1),
                    jnp.concatenate([edy_s[j, rows, :], edyl_s[rows, :]], axis=0),
                )
        for c in reversed(range(chunks)):
            rows = pl.ds(c * BLOCK, BLOCK)
            dy2 = dy_s[j, rows, :]
            mt2 = halves(
                jnp.concatenate([m_s[j, rows, k * BLOCK : (k + 1) * BLOCK].T for k in range(per)], axis=1)
            )
            dycat = [dy2[:, p * LANES : (p + 1) * LANES] * h for p in range(2) for h in half_b]
            bb = bb_s[rows, :]
            dstate = te_s[j, rows, :] * dot(
                bb, ds_s[j, rows, :]
            )
            mt3 = jnp.concatenate([mt2[:, : per * BLOCK], mt2], axis=1)
            dxd = dot(mt3, jnp.concatenate(dycat[per:] + dycat[:per] + dycat[:per], axis=0)) + dstate
            xa = xa_s[j, rows, :]
            dtp = dtp_s[j, rows, :]
            dy = dyf_s[rows, :]
            tail = jnp.sum(xa * dtp * dstate, axis=0, keepdims=True) + ea_s[
                j, pl.ds(c * BLOCK + BLOCK - 1, 1), :
            ] * jnp.sum(dsf_s[rows, :] * sin_s[j, rows, :], axis=0, keepdims=True)
            q = dxd * xa
            r = dy * y_s[j, rows, :] - q * dtp
            r = jnp.concatenate(
                [
                    r[: BLOCK - ROWS],
                    r[BLOCK - ROWS :] + jnp.where(iota(0, (ROWS, LANES)) == ROWS - 1, tail, 0.0),
                ],
                axis=0,
            )
            acc_s[rows, :] = acc_s[rows, :] + dot(halves(r), place_r) + dot(q.astype(BF16), place_q)
            du_s[j, rows, :] = (dxd * dtp + skips * dy) * gx_s[j, rows, :]
        return carry

    lax.fori_loop(0, pairs, middle, 0)

    acc_t = [acc_s[pl.ds(c * BLOCK, BLOCK), :].T for c in range(chunks)]
    dlogs = dot(
        halves(jnp.concatenate([t[0:ROWS] for t in acc_t], axis=0)), jnp.concatenate([tri, tri], axis=0)
    )
    ga = jnp.zeros((ROWS, LANES), F32)
    for c in range(chunks):
        rows = pl.ds(c * BLOCK, BLOCK)
        dlog = dlogs[c * ROWS : (c + 1) * ROWS]
        ddt = acc_t[c][LANES // 2 : LANES // 2 + ROWS] - dlog * decay
        dd_s[c] = (ddt * sig_s[:, rows]).astype(BF16)
        ga = ga + dlog * step_s[:, rows]
    for peer in sp_peers:
        d_copy(peer, sp).start()
    for peer in sp_peers:
        z_copy(peer, sp, pairs - 1).start()
    ga_col = jnp.sum(ga, axis=1, keepdims=True)

    def ga_row(col):
        diag = iota(0, (ROWS, heads)) == iota(1, (ROWS, heads))
        return jnp.sum(jnp.where(diag, jnp.broadcast_to(col, (ROWS, heads)), 0.0), axis=0, keepdims=True)

    def ga_copy(peer, recv):
        return remote(ga_s, rga.at[recv], ga_send.at[peer], ga_recv.at[recv], "dp", peer)

    if reduce_here:
        ga_s[...] = jnp.broadcast_to(ga_col, ga_s.shape)
        for peer in dp_peers:
            ga_copy(peer, dp).start()
    else:
        oga_ref[...] = ga_row(ga_col)

    def convolve(i, carry):
        c = chunks - 1 - i
        base = pl.multiple_of(c * BLOCK, BLOCK)
        rows = pl.ds(base, BLOCK)
        for j in range(pairs):
            cols = pl.ds(j * LANES, LANES)
            dx_s[j, rows, :] = conv_back(du_s.at[j], base, tapx_v[:, cols].astype(F32)).astype(BF16)
        return carry

    def backward(i, carry):
        c = chunks - 1 - i
        base = pl.multiple_of(c * BLOCK, BLOCK)
        rows = pl.ds(base, BLOCK)
        dscores = jnp.zeros((BLOCK, BLOCK), F32)
        dcc = jnp.zeros((BLOCK, STATE), F32)
        dbb = jnp.zeros((BLOCK, STATE), F32)
        for j in range(pairs):
            cols = pl.ds(j * LANES, LANES)
            xdb = xdb_s[j, rows, :]
            xcat = jnp.concatenate([xdb * h for h in half_b], axis=0)
            dm = dot(dy_s[j, rows, :], jnp.concatenate([xcat, xcat], axis=1), ROWS_ROWS) * lam_s[j, rows, :]
            for k in range(per):
                dscores = dscores + dm[:, k * BLOCK : (k + 1) * BLOCK]

        def joined(ref):
            return jnp.concatenate([ref[j, rows, :].astype(BF16) for j in range(pairs)], axis=1)

        dcc = dot(joined(edy_s), joined(sin_s), ROWS_ROWS)
        dbb = dot(joined(xdte_s), joined(ds_s), ROWS_ROWS)
        dcc = dcc + dot(dscores.astype(BF16), bb_s[rows, :])
        dbb = dbb + dot(dscores.T.astype(BF16), cb_s[rows, :])
        dbu_s[rows, :] = dbb * gb_s[rows, :]
        dcu_s[rows, :] = dcc * gc_s[rows, :]
        dbc_s[rows, 0:STATE] = conv_back(dbu_s, base, tapb_v[:, gcols].astype(F32)).astype(BF16)
        dbc_s[rows, STATE : 2 * STATE] = conv_back(dcu_s, base, tapc_v[:, gcols].astype(F32)).astype(BF16)
        return carry

    mid = chunks // 2
    lax.fori_loop(0, mid, backward, 0)

    rd[sp] = dd_s[sp]
    for peer in sp_peers:
        d_copy(peer, peer).wait_recv()
    whole_d = jnp.concatenate([rd[k].astype(F32)[:heads] for k in range(n_sp)], axis=0).astype(BF16)
    od_ref[...] = whole_d
    arrived("li")
    whole_w = dot(whole_d, li_v[...])

    if reduce_here:
        width = part.shape[1] // n_dp

        def w1_copy(peer, recv):
            return remote(
                part.at[:, block(peer, width)], rs1.at[recv], w1_send.at[peer], w1_recv.at[recv], "dp", peer
            )

        def w2_copy(peer, recv):
            return remote(mine1, rs2.at[recv], w2_send.at[peer], w2_recv.at[recv], "sp", peer)

        def w3_copy(peer, recv):
            return remote(mine2, rs3.at[recv], w3_send.at[peer], w3_recv.at[recv], "dp", peer)

        part[...] = whole_w.astype(BF16)
        for peer in dp_peers:
            w1_copy(peer, dp).start()
        rs1[dp] = part[:, block(dp, width)]
    else:
        ow_ref[...] = whole_w

    lax.fori_loop(0, chunks, convolve, 0)
    early = pairs // 2 if reduce_here else pairs
    for j in range(early):
        for peer in sp_peers:
            x_copy(peer, sp, j).start()

    lax.fori_loop(mid, chunks, backward, 0)

    if reduce_here:
        for peer in dp_peers:
            w1_copy(peer, peer).wait_recv()
        mine1[...] = add_all([rs1[k].astype(F32) for k in range(n_dp)]).astype(BF16)
        for peer in sp_peers:
            w2_copy(peer, sp).start()
        for j in range(early, pairs):
            for peer in sp_peers:
                x_copy(peer, sp, j).start()
        for peer in sp_peers:
            bc_copy(peer, sp).start()
        rs2[sp] = mine1[...]
        rga[dp] = ga_s[...]
        for peer in dp_peers:
            ga_copy(peer, peer).wait_recv()
        oga_ref[...] = ga_row(add_all([rga[k] for k in range(n_dp)])[:, 0:1])
        for peer in sp_peers:
            w2_copy(peer, peer).wait_recv()
        mine2[...] = add_all([rs2[k].astype(F32) for k in range(n_sp)]).astype(BF16)
        for peer in dp_peers:
            w3_copy(peer, dp).start()
        rs3[dp] = mine2[...]

    else:
        for peer in sp_peers:
            bc_copy(peer, sp).start()
    for j in range(pairs):
        oz_ref[:, block(sp * pairs + j, LANES)] = dz_s[j, ours, :]
        ox_ref[:, block(sp * pairs + j, LANES)] = dx_s[j, ours, :]
    rbc[sp] = dbc_s[ours, :]
    for peer in sp_peers:
        d_copy(peer, sp).wait_send()
        for j in range(pairs):
            cot_copy(peer, sp, j).wait_send()
            z_copy(peer, sp, j).wait_send()
            z_copy(peer, peer, j).wait_recv()
        for j in range(early):
            x_copy(peer, peer, j).wait_recv()
            x_copy(peer, sp, j).wait_send()
    for peer in dp_peers:
        ga_copy(peer, dp).wait_send()
        w1_copy(peer, dp).wait_send()
    for peer in sp_peers:
        if reduce_here:
            w2_copy(peer, sp).wait_send()
        for j in range(early, pairs):
            x_copy(peer, peer, j).wait_recv()
            x_copy(peer, sp, j).wait_send()
    for peer in sp_peers:
        bc_copy(peer, peer).wait_recv()
        bc_copy(peer, sp).wait_send()
    for g in range(GROUPS):
        total = add_all([rbc[g * group_span + k].astype(F32) for k in range(group_span)]).astype(BF16)
        ob_ref[:, g * STATE : (g + 1) * STATE] = total[:, 0:STATE]
        oc_ref[:, g * STATE : (g + 1) * STATE] = total[:, STATE : 2 * STATE]
    if reduce_here:
        for peer in dp_peers:
            w3_copy(peer, peer).wait_recv()
            w3_copy(peer, dp).wait_send()
        for k in range(n_dp):
            ow_ref[:, k * width : (k + 1) * width] = rs3[k].astype(F32)


def fused(args, n_sp, n_dp, group_span, head_dim, heads, reduce_here):
    cot, li, x, z, b, c, dt, tapx, tapb, tapc, bias, alog, skip, nw = args
    length, channels = x.shape
    tokens, width = li.shape
    all_heads = heads * n_sp
    per = LANES // head_dim
    pairs = channels // LANES
    vm = pltpu.VMEM
    dma = pltpu.SemaphoreType.DMA
    wide = vm((pairs, length, LANES), F32)
    wide_b = vm((pairs, length, LANES), BF16)
    thin = vm((length, LANES), F32)
    thin_b = vm((length, LANES), BF16)
    padded = vm((length + PAD, LANES), F32)
    tall = vm((pairs, length + PAD, LANES), F32)
    rows = vm((ROWS, length), F32)
    piece = width // n_dp if reduce_here else LANES
    return pl.pallas_call(
        functools.partial(step_kernel, n_sp, n_dp, group_span, head_dim, heads, reduce_here),
        out_shape=(
            jax.ShapeDtypeStruct((tokens, channels * n_sp), BF16),
            jax.ShapeDtypeStruct((tokens, channels * n_sp), BF16),
            jax.ShapeDtypeStruct((tokens, GROUPS * STATE), BF16),
            jax.ShapeDtypeStruct((tokens, GROUPS * STATE), BF16),
            jax.ShapeDtypeStruct((all_heads, tokens), BF16),
            jax.ShapeDtypeStruct((1, heads), F32),
            jax.ShapeDtypeStruct((all_heads, width), F32),
        ),
        in_specs=[pl.BlockSpec(memory_space=pltpu.MemorySpace.HBM)] * 14,
        out_specs=tuple([pl.BlockSpec(memory_space=pltpu.VMEM)] * 7),
        scratch_shapes=[
            vm((tokens, channels * n_sp), BF16),
            vm((tokens, width), BF16),
            wide_b,
            wide_b,
            thin_b,
            thin_b,
            vm((heads, length), BF16),
            vm(tapx.shape, BF16),
            vm(tapb.shape, BF16),
            vm(tapc.shape, BF16),
            vm((1, heads), F32),
            vm((1, heads), F32),
            vm((1, heads), F32),
            vm((1, channels), F32),
            wide_b,
            tall,
            padded,
            padded,
            wide,
            wide,
            wide,
            wide,
            wide,
            wide,
            wide,
            wide_b,
            vm((pairs, STATE, LANES), F32),
            vm((pairs, length, per * BLOCK), F32),
            vm((pairs, length, per * BLOCK), F32),
            wide_b,
            wide_b,
            vm((pairs, length, 2 * LANES), BF16),
            wide_b,
            tall,
            thin_b,
            thin_b,
            thin,
            thin,
            thin_b,
            padded,
            padded,
            vm((ROWS, channels), F32),
            rows,
            rows,
            vm((length // BLOCK * ROWS, LANES), F32),
            rows,
            vm((ROWS, LANES), F32),
            thin,
            thin,
            thin,
            thin_b,
            wide_b,
            wide_b,
            vm((length, 2 * STATE), BF16),
            vm((length // BLOCK, ROWS, BLOCK), BF16),
            vm((n_sp, tokens, 2 * STATE), BF16),
            vm((n_sp, ROWS, BLOCK), BF16),
            vm((n_dp, ROWS, LANES), F32),
            vm((all_heads, width), BF16),
            vm((n_dp, all_heads, piece), BF16),
            vm((all_heads, piece), BF16),
            vm((n_sp, all_heads, piece), BF16),
            vm((all_heads, piece), BF16),
            vm((n_dp, all_heads, piece), BF16),
            dma((12 + 2 * pairs,)),
        ]
        + [dma((n_sp, pairs))] * 6
        + [dma((n_sp,))] * 4
        + [dma((n_dp,))] * 4
        + [dma((n_sp,))] * 2
        + [dma((n_dp,))] * 2,
        compiler_params=pltpu.CompilerParams(
            collective_id=0, has_side_effects=True, vmem_limit_bytes=40 * 1024 * 1024
        ),
    )(*args)


def out_kernel(count, *refs):
    srcs, dsts, sem = refs[:count], refs[count : 2 * count], refs[2 * count]
    copies = [pltpu.make_async_copy(s, d, sem.at[k]) for k, (s, d) in enumerate(zip(srcs, dsts))]
    for copy in copies:
        copy.start()
    for copy in copies:
        copy.wait()


def copy_out(arrays):
    n = len(arrays)
    return pl.pallas_call(
        functools.partial(out_kernel, n),
        out_shape=tuple(jax.ShapeDtypeStruct(a.shape, a.dtype) for a in arrays),
        in_specs=[pl.BlockSpec(memory_space=pltpu.VMEM)] * n,
        out_specs=tuple([pl.BlockSpec(memory_space=pltpu.MemorySpace.HBM)] * n),
        scratch_shapes=[pltpu.SemaphoreType.DMA((n,))],
        compiler_params=pltpu.CompilerParams(vmem_limit_bytes=1024 * 1024),
    )(*arrays)


def shards(
    cotangent,
    layer_input,
    x_pre,
    z_pre,
    b_pre,
    c_pre,
    dt_raw,
    conv_x,
    conv_b,
    conv_c,
    dt_bias,
    a_log,
    d_skip,
    norm_w,
):
    n_sp = lax.axis_size("sp")
    n_dp = lax.axis_size("dp")
    assert x_pre.shape[0] == 1
    assert cotangent.shape[1] == BLOCK
    heads_here = dt_raw.shape[2]
    heads = heads_here * n_sp
    head_dim = x_pre.shape[2] // heads_here
    group_span = n_sp // GROUPS
    reduce_here = heads % 16 == 0 and (layer_input.shape[2] // n_dp) % LANES == 0
    args = (
        cotangent[0],
        layer_input[0],
        x_pre[0],
        z_pre[0],
        b_pre[0],
        c_pre[0],
        dt_raw[0].T,
        conv_x,
        conv_b,
        conv_c,
        dt_bias[None],
        a_log[None],
        d_skip[None],
        norm_w[None],
    )
    args = tuple(pltpu.with_memory_space_constraint(a, pltpu.MemorySpace.HBM) for a in args)
    ox, oz, ob, oc, od, oga, ow = copy_out(
        fused(args, n_sp, n_dp, group_span, head_dim, heads_here, reduce_here)
    )
    grad_a_log = oga[0]
    if not reduce_here:
        ow, grad_a_log = lax.psum((ow, grad_a_log), "dp")
        ow = lax.psum(ow, "sp")
    return ox[None], oz[None], ob[None], oc[None], od.T[None], grad_a_log, ow.T


def solution(mesh):
    placed = (
        P("dp", "sp", None),
        P("dp", "sp", None),
        P("dp", None, "sp"),
        P("dp", None, "sp"),
        P("dp", None, None),
        P("dp", None, None),
        P("dp", None, "sp"),
        P(None, "sp"),
        P(),
        P(),
        P("sp"),
        P("sp"),
        P("sp"),
        P("sp"),
    )
    return jax.shard_map(
        shards,
        mesh=mesh,
        in_specs=placed,
        out_specs=(
            P("dp", "sp", None),
            P("dp", "sp", None),
            P("dp", "sp", None),
            P("dp", "sp", None),
            P("dp", "sp", None),
            P("sp"),
            P(),
        ),
        check_vma=False,
    )
```
